32 devices in a mesh: sp: 8 (over z, x), tp: 4 (over y, core).
Axes of the slice: x: 2, y: 2, z: 4, core: 2. Of those that a mesh axis runs over, the one named last changes fastest.
Arguments:
- latent: bfloat16 [4096, 4096], P('sp'), may hold values from -64 to 64
- context: bfloat16 [512, 4096], P('sp'), may hold values from -6 to 6
- condition: bfloat16 [4096], P('sp'), may hold values from -6 to 6
- context_condition: bfloat16 [4096], P('sp'), may hold values from -6 to 6
- shift_weight: bfloat16 [4096, 4096], P('sp', 'tp'), may hold values from -0.125 to 0.125
- scale_weight: bfloat16 [4096, 4096], P('sp', 'tp'), may hold values from -0.125 to 0.125
- gate_weight: bfloat16 [4096, 4096], P('sp', 'tp'), may hold values from -0.25 to 0.25
- norm_gain: float32 [4096], replicated, may hold values from 0.1 to 1.9
- query_weight: bfloat16 [4096, 2048], P(None, 'tp'), may hold values from -0.09375 to 0.09375
- key_weight: bfloat16 [4096, 2048], P(None, 'tp'), may hold values from -0.09375 to 0.09375
- value_weight: bfloat16 [4096, 2048], P(None, 'tp'), may hold values from -0.09375 to 0.09375
- write_weight: bfloat16 [4096, 2, 16], replicated, may hold values from -0.09375 to 0.09375
- decay_weight: bfloat16 [4096, 2, 16], replicated, may hold values from -0.09375 to 0.09375
- write_bias: float32 [2, 16], replicated, may hold values from -12 to 1
- decay_bias: float32 [2, 16], replicated, may hold values from -16 to -4
- log_rate: float32 [2, 16], replicated, may hold values from 0 to 1.4
- head_gain: float32 [128], replicated, may hold values from 0.1 to 1.9
- out_weight: bfloat16 [2048, 4096], P(None, 'tp'), may hold values from -0.125 to 0.125
Outputs:
- updated: bfloat16 [4096, 4096], P('sp', 'tp')
The draws below stay inside these ranges and needn't reach their ends.
All inputs are finite; a program needn't handle non-finite values.
Results may differ from the reference program's by a relative error of at most 0.013.
Values may be sent and summed in bfloat16 or wider, within the bound.
A program may use at most 128 MiB of HBM per device.

```python
import math
import jax
import jax.numpy as jnp
from jax import lax

D = 4096
HEADS = 16
HEAD_DIM = 128
BLOCK = 64
TOKENS = 4096
CTX = 512


def draw_latent(key, part):
    segment_count = (TOKENS + 127) // 128
    offsets = jnp.clip(jax.random.normal(jax.random.fold_in(key, 22), (segment_count, D), jnp.float32), -3.0, 3.0)
    segment_index = jnp.arange(TOKENS) // 128
    noise = jnp.clip(jax.random.normal(jax.random.fold_in(key, 21), (TOKENS, D), jnp.float32), -6.0, 6.0)
    return (noise + offsets[segment_index]).astype(jnp.bfloat16)


def head_speeds(key):
    chooser = jax.random.uniform(jax.random.fold_in(key, 31), (2, HEADS), jnp.float32)
    return chooser < 0.7


def draw_decay_bias(key, part):
    keeping = head_speeds(key)
    spread = jax.random.uniform(jax.random.fold_in(key, 32), (2, HEADS), jnp.float32, -0.5, 0.5)
    slow_value = math.log(0.05 / (TOKENS + CTX)) + spread
    fast_value = -5.0 + spread
    return jnp.where(keeping, slow_value, fast_value).astype(jnp.float32)


def draw_write_bias(key, part):
    keeping = head_speeds(key)
    spread = jax.random.uniform(jax.random.fold_in(key, 33), (2, HEADS), jnp.float32, -0.5, 0.5)
    slow_value = math.log(HEAD_DIM / (TOKENS + CTX)) - 1.5 + spread
    fast_value = spread
    return jnp.where(keeping, slow_value, fast_value).astype(jnp.float32)


def block_levels(rng, shape, cuts, least, high):
    level = 1.0
    for position, blocks in cuts:
        draws = jax.random.uniform(jax.random.fold_in(jax.random.fold_in(rng, 6), position), (blocks,), jnp.float32, least / len(cuts), high / len(cuts))
        level = level * jnp.repeat(jnp.exp(draws), shape[position] // blocks).reshape((-1,) + (1,) * (len(shape) - 1 - position))
    return level


def gaussian(key, extent, scale, most, split=(), held_as=jnp.bfloat16):
    drawn = jax.random.normal(key, extent, jnp.float32) * scale
    if len(split) > 0:
        drawn = block_levels(key, extent, split, -0.22, 0.18) * drawn
    return jnp.clip(drawn, min=-most, max=most).astype(held_as)


def setup_inputs(seed: int = 0) -> dict:
    keys = jax.random.split(jax.random.key(seed), 19)
    return {
        "latent": draw_latent(jax.random.fold_in(keys[18], 71), 0),
        "context": gaussian(keys[1], (CTX, D), 1.0, 6.0, ((0, 8),)),
        "condition": gaussian(keys[2], (D,), 1.0, 6.0, ((0, 8),)),
        "context_condition": gaussian(keys[3], (D,), 1.0, 6.0, ((0, 8),)),
        "shift_weight": gaussian(keys[4], (D, D), (D // 2) ** -0.5, 0.125, ((0, 8), (1, 4))),
        "scale_weight": gaussian(keys[5], (D, D), (D // 2) ** -0.5, 0.125, ((0, 8), (1, 4))),
        "gate_weight": gaussian(keys[6], (D, D), (D // 8) ** -0.5, 0.25, ((0, 8), (1, 4))),
        "norm_gain": jnp.clip(1.0 + 0.18 * jax.random.normal(keys[7], (D,), jnp.float32), 0.1, 1.9),
        "query_weight": gaussian(keys[8], (D, HEADS * HEAD_DIM), D ** -0.5, 0.09375, ((1, 4),)),
        "key_weight": gaussian(keys[9], (D, HEADS * HEAD_DIM), D ** -0.5, 0.09375, ((1, 4),)),
        "value_weight": gaussian(keys[10], (D, HEADS * HEAD_DIM), D ** -0.5, 0.09375, ((1, 4),)),
        "write_weight": gaussian(keys[11], (D, 2, HEADS), D ** -0.5, 0.09375),
        "decay_weight": gaussian(keys[12], (D, 2, HEADS), D ** -0.5, 0.09375),
        "write_bias": draw_write_bias(jax.random.fold_in(keys[18], 71), 0),
        "decay_bias": draw_decay_bias(jax.random.fold_in(keys[18], 71), 0),
        "log_rate": jnp.clip(jax.random.uniform(keys[15], (2, HEADS), jnp.float32, 0.0, 1.4), 0.0, 1.4),
        "head_gain": jnp.clip(1.0 + 0.18 * jax.random.normal(keys[16], (HEAD_DIM,), jnp.float32), 0.1, 1.9),
        "out_weight": gaussian(keys[17], (HEADS * HEAD_DIM, D), (HEADS * HEAD_DIM) ** -0.5, 0.125, ((1, 4),)),
    }


epsilon = 0.0001
highest = lax.Precision.HIGHEST

def rms_rows(row_data, row_gain):
    values = row_data.astype(jnp.float32)
    scaled = values * lax.rsqrt(lax.optimization_barrier(jnp.mean(values * values, axis=-1, keepdims=True)) + epsilon)
    return scaled * row_gain.astype(jnp.float32)

def unit_heads(matrix, head_count):
    split_heads = matrix.astype(jnp.float32).reshape(matrix.shape[0], head_count, -1)
    return split_heads * lax.rsqrt(lax.optimization_barrier(jnp.sum(split_heads * split_heads, axis=-1, keepdims=True)) + epsilon)

def head_gates(write_pre, decay_pre, write_bias, decay_bias, log_rate):
    write_rate = jax.nn.sigmoid(write_pre.astype(jnp.float32) + write_bias)
    log_decay = -jnp.exp(log_rate) * jax.nn.softplus(decay_pre.astype(jnp.float32) + decay_bias)
    return (write_rate, log_decay)

def project(matrix, weight):
    return jnp.dot(matrix.astype(jnp.float32), weight.astype(jnp.float32), preferred_element_type=jnp.float32).astype(jnp.bfloat16)

def to_blocks(source):
    heads_first = jnp.moveaxis(source, 1, 0)
    block_count = heads_first.shape[1] // BLOCK
    return heads_first.reshape((heads_first.shape[0], block_count, BLOCK) + heads_first.shape[2:])

def prepare_keys(key_vecs, value_vecs, log_decay, write_rate):
    block_keys = to_blocks(key_vecs)
    block_values = to_blocks(value_vecs)
    running = jnp.cumsum(to_blocks(log_decay), axis=-1)
    block_rates = to_blocks(write_rate)
    offsets = jnp.arange(BLOCK)
    lower_mask = offsets[:, None] >= offsets[None, :]
    strict_mask = offsets[:, None] > offsets[None, :]
    spread = running[..., :, None] - running[..., None, :]
    decay_mat = jnp.where(lower_mask, jnp.exp(jnp.where(lower_mask, spread, 0.0)), 0.0)
    scaled = block_keys * block_rates[..., None]
    system = jnp.einsum('hnid,hnjd->hnij', scaled, block_keys, precision=highest) * decay_mat
    system = jnp.where(strict_mask, system, 0.0) + jnp.eye(BLOCK, dtype=system.dtype)
    fresh_values = jax.scipy.linalg.solve_triangular(system, block_values * block_rates[..., None], lower=True, unit_diagonal=True)
    key_weights = jax.scipy.linalg.solve_triangular(system, scaled * jnp.exp(running)[..., None], lower=True, unit_diagonal=True)
    last_gate = running[..., -1]
    late_keys = block_keys * jnp.exp(last_gate[..., None] - running)[..., None]
    return (block_keys, running, decay_mat, fresh_values, key_weights, last_gate, late_keys)

def prepare_queries(query_vecs, prepared):
    block_queries = to_blocks(query_vecs)
    query_keys = jnp.einsum('hnid,hnjd->hnij', block_queries, prepared[0], precision=highest) * prepared[2]
    early_queries = block_queries * jnp.exp(prepared[1])[..., None]
    return (query_keys, early_queries)

def run_blocks(prepared, queried, start):
    inputs = tuple((jnp.moveaxis(item, 1, 0) for item in (prepared[3], prepared[4], queried[0], queried[1], prepared[6], prepared[5])))

    def advance(carried, pieces):
        new_in, key_in, score_in, query_in, late_in, gate_in = pieces
        corrected = new_in - jnp.einsum('hcd,hde->hce', key_in, carried, precision=highest)
        output = jnp.einsum('hcd,hde->hce', query_in, carried, precision=highest)
        output = output + jnp.einsum('hij,hje->hie', score_in, corrected, precision=highest)
        carried = carried * jnp.exp(gate_in)[:, None, None] + jnp.einsum('hcd,hce->hde', late_in, corrected, precision=highest)
        return (carried, output)
    closing, outputs = lax.scan(advance, start, inputs)
    merged = jnp.transpose(outputs, (0, 2, 1, 3))
    return merged.reshape(-1, merged.shape[2], merged.shape[3])

def final_state(prepared, start):
    inputs = tuple((jnp.moveaxis(item, 1, 0) for item in (prepared[3], prepared[4], prepared[6], prepared[5])))

    def advance(carried, pieces):
        new_in, key_in, late_in, gate_in = pieces
        corrected = new_in - jnp.einsum('hcd,hde->hce', key_in, carried, precision=highest)
        carried = carried * jnp.exp(gate_in)[:, None, None] + jnp.einsum('hcd,hce->hde', late_in, corrected, precision=highest)
        return (carried, None)
    closing, unused = lax.scan(advance, start, inputs)
    return closing

def reference(latent, context, condition, context_condition, shift_weight, scale_weight, gate_weight, norm_gain, query_weight, key_weight, value_weight, write_weight, decay_weight, write_bias, decay_bias, log_rate, head_gain, out_weight):
    head_count = write_bias.shape[1]
    width = write_weight.shape[0]
    stacked = jnp.stack([condition, context_condition]).astype(jnp.float32)
    silu_rows = jax.nn.silu(stacked).astype(jnp.bfloat16)
    shift_rows = jnp.dot(silu_rows.astype(jnp.float32), shift_weight.astype(jnp.float32), preferred_element_type=jnp.float32)
    scale_rows = jnp.dot(silu_rows.astype(jnp.float32), scale_weight.astype(jnp.float32), preferred_element_type=jnp.float32)
    gate_row = jnp.dot(silu_rows[0].astype(jnp.float32), gate_weight.astype(jnp.float32), preferred_element_type=jnp.float32)
    modulated = (rms_rows(latent, norm_gain) * (1.0 + scale_rows[0]) + shift_rows[0]).astype(jnp.bfloat16)
    ctx_modulated = (rms_rows(context, norm_gain) * (1.0 + scale_rows[1]) + shift_rows[1]).astype(jnp.bfloat16)
    write_flat = write_weight.reshape(width, -1)
    decay_flat = decay_weight.reshape(width, -1)
    ctx_keys = unit_heads(project(ctx_modulated, key_weight), head_count)
    ctx_values = project(ctx_modulated, value_weight).astype(jnp.float32).reshape(-1, head_count, HEAD_DIM)
    ctx_rate, ctx_log = head_gates(project(ctx_modulated, write_flat).reshape(-1, 2, head_count), project(ctx_modulated, decay_flat).reshape(-1, 2, head_count), write_bias, decay_bias, log_rate)
    start_zero = jnp.zeros((head_count, HEAD_DIM, HEAD_DIM), jnp.float32)
    ctx_forward = final_state(prepare_keys(ctx_keys, ctx_values, ctx_log[:, 0], ctx_rate[:, 0]), start_zero)
    ctx_backward = final_state(prepare_keys(jnp.flip(ctx_keys, 0), jnp.flip(ctx_values, 0), jnp.flip(ctx_log[:, 1], 0), jnp.flip(ctx_rate[:, 1], 0)), start_zero)
    queries = unit_heads(project(modulated, query_weight), head_count) * HEAD_DIM ** (-0.5)
    key_vecs = unit_heads(project(modulated, key_weight), head_count)
    value_vecs = project(modulated, value_weight).astype(jnp.float32).reshape(-1, head_count, HEAD_DIM)
    write_rate, log_decay = head_gates(project(modulated, write_flat).reshape(-1, 2, head_count), project(modulated, decay_flat).reshape(-1, 2, head_count), write_bias, decay_bias, log_rate)
    forward_prep = prepare_keys(key_vecs, value_vecs, log_decay[:, 0], write_rate[:, 0])
    forward_out = run_blocks(forward_prep, prepare_queries(queries, forward_prep), ctx_forward)
    backward_prep = prepare_keys(jnp.flip(key_vecs, 0), jnp.flip(value_vecs, 0), jnp.flip(log_decay[:, 1], 0), jnp.flip(write_rate[:, 1], 0))
    backward_out = jnp.flip(run_blocks(backward_prep, prepare_queries(jnp.flip(queries, 0), backward_prep), ctx_backward), 0)
    combined = forward_out + backward_out
    head_out = combined * lax.rsqrt(lax.optimization_barrier(jnp.mean(combined * combined, axis=-1, keepdims=True)) + epsilon) * head_gain.astype(jnp.float32)
    head_out = head_out.astype(jnp.bfloat16).reshape(combined.shape[0], -1)
    branch = jnp.dot(head_out.astype(jnp.float32), out_weight.astype(jnp.float32), preferred_element_type=jnp.float32)
    return (latent.astype(jnp.float32) + gate_row * branch).astype(jnp.bfloat16)
```

```python
import functools

import jax
import jax.numpy as jnp
from jax import lax
from jax.experimental import pallas as pl
from jax.experimental.pallas import tpu as pltpu
from jax.sharding import PartitionSpec as P

HEAD_DIM = 128
CHUNK = 128
epsilon = 0.0001
bf16 = jnp.bfloat16
f32 = jnp.float32


def mm(a, b):
    return jnp.dot(a.astype(bf16), b.astype(bf16), preferred_element_type=f32)


def on_mesh(sp=None, tp=None):
    return (lax.axis_index("sp") if sp is None else sp, lax.axis_index("tp") if tp is None else tp)


def send(src, dst, send_sem, recv_sem, device):
    return pltpu.make_async_remote_copy(
        src_ref=src,
        dst_ref=dst,
        send_sem=send_sem,
        recv_sem=recv_sem,
        device_id=device,
        device_id_type=pl.DeviceIdType.MESH,
    )


def greet(devices):
    barrier = pltpu.get_barrier_semaphore()
    for device in devices:
        pl.semaphore_signal(barrier, inc=1, device_id=device, device_id_type=pl.DeviceIdType.MESH)


def grid_iota(size):
    return (
        lax.broadcasted_iota(jnp.int32, (size, size), 0),
        lax.broadcasted_iota(jnp.int32, (size, size), 1),
    )


def start_inverse(item, rows, cols):
    near = (rows // 2) == (cols // 2)
    item["inv"] = jnp.where(rows == cols, 1.0, jnp.where(near, -item["system"], 0.0))


def finish_inverse(items, size):
    span = 2
    while span < size:
        firsts = []
        for item in items:
            late, early = item["late_axis"] // span, item["early_axis"] // span
            mask = ((late % 2) == 1) & (early == late - 1)
            firsts.append(mm(jnp.where(mask, item["system"], 0.0), item["inv"]))
        for item, first in zip(items, firsts):
            item["inv"] = item["inv"] - mm(item["inv"], first)
        span *= 2


def key_grams(keys):
    size = keys.shape[0]
    rows, cols = grid_iota(size)
    keys_t = keys.astype(f32).T
    gram = jnp.dot(keys, keys_t.astype(bf16), preferred_element_type=f32)
    diag = jnp.where(rows == cols, gram, 0.0)
    s_col = lax.rsqrt(jnp.sum(diag, axis=1, keepdims=True) + epsilon)
    s_row = lax.rsqrt(jnp.sum(diag, axis=0, keepdims=True) + epsilon)
    return gram * s_col * s_row, keys.astype(f32) * s_col, keys_t * s_row, s_row


def eye_matrix():
    rows, cols = grid_iota(HEAD_DIM)
    return (rows == cols).astype(f32)


def prepare_maps(tokens, span, k_ref, v_ref, col_ref, row_ref, srow_ref, solved_ref, carry_ref, map_ref):
    size = min(CHUNK, tokens)
    rows, cols = grid_iota(size)
    items = []
    shared = []
    for at in range(0, tokens, size):
        gram, keys, keys_t, s_row = key_grams(k_ref[at : at + size, :])
        srow_ref[:, at : at + size] = s_row
        shared.append((keys, keys_t, v_ref[at : at + size, :].astype(f32)))
        for d in range(2):
            rate_col = col_ref[at : at + size, span * d : span * d + 1]
            run_col = col_ref[at : at + size, span * (2 + d) : span * (2 + d) + 1]
            run_row = row_ref[2 + d : 3 + d, at : at + size]
            strict = rows > cols if d == 0 else rows < cols
            decay = jnp.where(strict, jnp.exp(jnp.minimum(run_col - run_row, 0.0)), 0.0)
            item = dict(at=at, d=d, rate_col=rate_col, run_col=run_col, run_row=run_row)
            item["system"] = gram * decay * rate_col
            item["late_axis"], item["early_axis"] = (rows, cols) if d == 0 else (cols, rows)
            start_inverse(item, rows, cols)
            items.append(item)
    finish_inverse(items, size)
    for item in items:
        keys, keys_t, values = shared[item["at"] // size]
        growth = jnp.exp(item["run_col"])
        both = jnp.concatenate([values * item["rate_col"], keys * (item["rate_col"] * growth)], axis=1)
        solved = mm(item["inv"], both).astype(bf16)
        solved_ref[item["at"] // size, item["d"]] = solved
        last = item["run_row"][:, size - 1 :] if item["d"] == 0 else item["run_row"][:, :1]
        item["gate"] = jnp.exp(last)
        item["late"] = mm(keys_t * jnp.exp(last - item["run_row"]), solved)
    eye = eye_matrix()
    for d in range(2):
        chunks = [i for i in items if i["d"] == d]
        carry = None
        for item in chunks if d == 0 else chunks[::-1]:
            late, gate = item["late"], item["gate"]
            fresh = jnp.concatenate([late[:, :HEAD_DIM], (gate - 1.0) * eye - late[:, HEAD_DIM:]], axis=1)
            if carry is None:
                carry = fresh
            else:
                held = carry.astype(bf16)
                carry_ref[item["at"] // size, d] = held
                carry = gate * carry + fresh - mm(late[:, HEAD_DIM:], held)
        map_ref[d] = carry.astype(bf16)


def prepare_outputs(tokens, span, q_ref, k_ref, col_ref, row_ref, srow_ref, solved_ref, carry_ref, o_ref, e_ref):
    size = min(CHUNK, tokens)
    rows, cols = grid_iota(size)
    count = tokens // size
    for index in range(count):
        at = index * size
        raw = q_ref[at : at + size, :]
        queries = raw.astype(f32)
        q_scale = lax.rsqrt(jnp.sum(queries * queries, axis=1, keepdims=True) + epsilon) * HEAD_DIM**-0.5
        queries = queries * q_scale
        score = lax.dot_general(
            raw, k_ref[at : at + size, :], (((1,), (1,)), ((), ())), preferred_element_type=f32
        ) * (q_scale * srow_ref[:, at : at + size])
        total = None
        for d in range(2):
            run_col = col_ref[at : at + size, span * (2 + d) : span * (2 + d) + 1]
            run_row = row_ref[2 + d : 3 + d, at : at + size]
            inside = rows >= cols if d == 0 else rows <= cols
            decay = jnp.where(inside, jnp.exp(jnp.minimum(run_col - run_row, 0.0)), 0.0)
            weighed = mm(score * decay, solved_ref[index, d])
            local = weighed[:, :HEAD_DIM]
            early = queries * jnp.exp(run_col) - weighed[:, HEAD_DIM:]
            if index != (0 if d == 0 else count - 1):
                moved = mm(early, carry_ref[index, d])
                local = local + moved[:, :HEAD_DIM]
                early = early + moved[:, HEAD_DIM:]
            e_ref[at : at + size, d * HEAD_DIM : (d + 1) * HEAD_DIM] = early.astype(bf16)
            total = local if total is None else total + local
        o_ref[at : at + size, :] = total


def context_state(places, d, k_ref, v_ref, g_ref):
    size = k_ref.shape[1]
    rows, cols = grid_iota(size)
    items = []
    for step in range(places):
        place = step + d * (places - 1 - 2 * step)
        gram, keys, keys_t, unused = key_grams(k_ref[place])
        gates = g_ref[place]
        gates_t = gates.T
        rate_col, run_col, run_row = gates_t[:size, 0:1], gates_t[:size, 1:2], gates[1:2, :size]
        item = dict(keys=keys, keys_t=keys_t, values=v_ref[place].astype(f32), rate_col=rate_col)
        item["run_col"], item["run_row"] = run_col, run_row
        item["late_axis"] = jnp.where(d == 0, rows, cols)
        item["early_axis"] = jnp.where(d == 0, cols, rows)
        strict = item["late_axis"] > item["early_axis"]
        decay = jnp.where(strict, jnp.exp(jnp.minimum(run_col - run_row, 0.0)), 0.0)
        item["system"] = gram * decay * rate_col
        start_inverse(item, rows, cols)
        items.append(item)
    finish_inverse(items, size)
    for item in items:
        growth = jnp.exp(item["run_col"])
        both = jnp.concatenate(
            [item["values"] * item["rate_col"], item["keys"] * (item["rate_col"] * growth)], axis=1
        )
        solved = mm(item["inv"], both)
        run_row = item["run_row"]
        last = jnp.where(d == 0, run_row[:, size - 1 :], run_row[:, :1])
        item["gate"] = jnp.exp(last)
        item["late"] = mm(item["keys_t"] * jnp.exp(last - run_row), solved)
    state = items[0]["late"][:, :HEAD_DIM]
    for item in items[1:]:
        late = item["late"]
        state = item["gate"] * state + late[:, :HEAD_DIM] - mm(late[:, HEAD_DIM:], state)
    return state


def log1p_unit(u):
    z = u / (2.0 + u)
    z2 = z * z
    series = 1.0 / 11.0 + 0.0 * z2
    for power in (9, 7, 5, 3, 1):
        series = series * z2 + 1.0 / power
    return 2.0 * z * series


def triangle_sums(lower, parts):
    return sum(jnp.dot(lower, part, preferred_element_type=f32) for part in parts)


def split_three(values):
    high = values.astype(bf16)
    rest = values - high.astype(f32)
    middle = rest.astype(bf16)
    return high, middle, (rest - middle.astype(f32)).astype(bf16)


def mixer_kernel(
    sp, tp, heads, per,
    cond_ref, ctx_cond_ref, gain_ref, head_gain_ref, wb_ref, db_ref, lr_ref,
    shift_ref, scale_ref, gate_ref, latent_ref, context_ref, write_ref, decay_ref,
    wq_ref, wk_ref, wv_ref, wo_ref,
    out_ref,
    mod_w, rows_in, weights, gate_w, wo, rstd, mixed, q_s, k_s, v_s,
    got, blocks, gate_row, cols, rows_g, srow, solved, carry, maps, o_s, e_s,
    ctx_send, ctx_k, ctx_v, ctx_g, s_zero, got_map, pair_map, start_in, start_own, hop_out, ho, acc,
    local_sems, sent_a, recv_a, sent_b, recv_b, sent_c, recv_c, sent_s, recv_s, sent_m, recv_m,
    sent_h, sent_y, recv_y, sent_p, recv_p, sent_r, recv_r,
):
    me, col = lax.axis_index("sp"), lax.axis_index("tp")
    width = shift_ref.shape[1]
    tokens, ctx_tokens = latent_ref.shape[0], context_ref.shape[0]
    total_rows = tokens + ctx_tokens
    depth = latent_ref.shape[1]
    out_width = heads * HEAD_DIM
    items = 2 * heads
    loads = []

    def load(src, dst):
        loads.append(pltpu.make_async_copy(src, dst, local_sems.at[len(loads)]))
        loads[-1].start()
        return loads[-1]

    mods = [load(ref, mod_w.at[i]) for i, ref in enumerate([shift_ref, scale_ref, gate_ref])]
    acts = [
        load(context_ref, rows_in.at[pl.ds(tokens, ctx_tokens)]),
        load(latent_ref, rows_in.at[pl.ds(0, tokens)]),
    ]
    gate_rows = write_ref.shape[0]
    projs = [
        load(write_ref, gate_w.at[pl.ds(0, gate_rows)]),
        load(decay_ref, gate_w.at[pl.ds(gate_rows, gate_rows)]),
    ]
    projs += [
        load(ref, weights.at[:, pl.ds(i * out_width, out_width)]) for i, ref in enumerate([wk_ref, wv_ref, wq_ref])
    ]
    out_load = load(wo_ref, wo)
    rings = [on_mesh(sp=lax.rem(me + r, sp)) for r in range(1, sp)]
    cross = [on_mesh(tp=lax.rem(col + r, tp)) for r in range(1, tp)]
    greet(rings + cross)

    def flat(ref):
        values = ref[...].astype(f32)
        return jnp.concatenate([values[i : i + 1] for i in range(values.shape[0])], axis=1)

    silu = jnp.concatenate([flat(cond_ref), flat(ctx_cond_ref), jnp.zeros((6, cond_ref.size), f32)], axis=0)
    silu = (silu / (1.0 + jnp.exp(-silu))).astype(bf16)
    parts = []
    for i in range(3):
        mods[i].wait()
        parts.append(jnp.dot(silu, mod_w[i], preferred_element_type=f32))
    got[me] = jnp.concatenate(
        [parts[0][0:2], parts[1][0:2], parts[2][0:1], jnp.zeros((3, width), f32)], axis=0
    ).astype(bf16)
    pl.semaphore_wait(pltpu.get_barrier_semaphore(), len(rings) + len(cross))
    out = []
    for r, device in enumerate(rings):
        out.append(send(got.at[me], got.at[me], sent_a.at[r], recv_a.at[me], device))
        out[-1].start()
    for act in acts:
        act.wait()
    step = 16

    def stats(i, unused):
        at = pl.ds(pl.multiple_of(i * step, step), step)
        values = rows_in[at, :].astype(f32)
        mean = jnp.sum(values * values, axis=1, keepdims=True) * (1.0 / depth)
        rstd[at, :] = jnp.broadcast_to(lax.rsqrt(mean + epsilon), (step, 128))
        return unused

    lax.fori_loop(0, total_rows // step, stats, 0)
    for r in range(1, sp):
        src = lax.rem(me + r, sp)
        send(got.at[src], got.at[src], sent_a.at[0], recv_a.at[src], on_mesh(sp=src)).wait_recv()
    summed = got[0].astype(f32)
    for place in range(1, sp):
        summed = summed + got[place].astype(f32)
    blocks[col] = summed[0:4]
    gate_row[...] = summed[4:5]
    for r, device in enumerate(cross):
        out.append(send(blocks.at[col], blocks.at[col], sent_b.at[r], recv_b.at[col], device))
        out[-1].start()
    for r in range(1, tp):
        src = lax.rem(col + r, tp)
        send(blocks.at[src], blocks.at[src], sent_b.at[0], recv_b.at[src], on_mesh(tp=src)).wait_recv()

    def modulate_rows(start, count, index):
        for place in range(tp):
            lanes = slice(place * width, (place + 1) * width)
            block = blocks[place]
            slope = gain_ref[:, lanes] * (1.0 + block[2 + index : 3 + index])
            shift = block[index : index + 1]

            def modulate(i, unused):
                at = pl.ds(pl.multiple_of(start + i * step, step), step)
                scale = jnp.concatenate([rstd[at, :]] * (width // 128), axis=1)
                mixed[at, lanes] = (rows_in[at, lanes].astype(f32) * scale * slope + shift).astype(bf16)
                return unused

            lax.fori_loop(0, count // step, modulate, 0)

    tile = 256 if out_width % 256 == 0 else 128

    def project(first, count, which, ref, base):
        def columns(j, unused):
            lanes = pl.ds(pl.multiple_of(which * out_width + j * tile, tile), tile)
            part = jnp.dot(mixed[pl.ds(first, count), :], weights[:, lanes], preferred_element_type=f32)
            ref[pl.ds(first, count), pl.ds(pl.multiple_of(j * tile, tile), tile)] = part.astype(bf16)
            return unused

        lax.fori_loop(0, out_width // tile, columns, 0)

    first_head = col * heads
    span = wb_ref.shape[1]
    bias = jnp.concatenate([wb_ref[0:1], wb_ref[1:2], db_ref[0:1], db_ref[1:2]], axis=1)
    rates = jnp.concatenate([lr_ref[0:1], lr_ref[1:2]] * 2, axis=1)
    lanes_here = bias.shape[1]

    def make_gates(first, count, size):
        pre = lax.dot_general(
            mixed[pl.ds(first, count), :], gate_w[...], (((1,), (1,)), ((), ())), preferred_element_type=f32
        ).astype(bf16).astype(f32) + bias
        rate = 1.0 / (1.0 + jnp.exp(-pre))
        decay = -jnp.exp(rates) * (jnp.maximum(pre, 0.0) + log1p_unit(jnp.exp(-jnp.abs(pre))))
        lane = lax.broadcasted_iota(jnp.int32, (count, lanes_here), 1)
        rows, columns = grid_iota(size)
        lower, upper = (rows >= columns).astype(bf16), (rows <= columns).astype(bf16)
        backward = lax.broadcasted_iota(jnp.int32, (size, lanes_here), 1) >= 3 * span
        running = []
        for at in range(0, count, size):
            split = split_three(decay[at : at + size])
            running.append(jnp.where(backward, triangle_sums(upper, split), triangle_sums(lower, split)))
        gates = jnp.where(lane < 2 * span, rate, jnp.concatenate(running, axis=0))
        gates = jnp.concatenate([gates, jnp.zeros((count, 128 - lanes_here), f32)], axis=1)
        gates = pltpu.roll(gates, lax.rem(128 - first_head, 128), 1)
        for head in range(heads):
            cols[head, pl.ds(first, count), :] = gates if head == 0 else pltpu.roll(gates, 128 - head, 1)
        return gates

    for proj in projs[:2]:
        proj.wait()
    modulate_rows(tokens, ctx_tokens, 1)
    ctx_gates = make_gates(tokens, ctx_tokens, ctx_tokens)
    if ctx_tokens < 128:
        ctx_gates = jnp.concatenate([ctx_gates, jnp.zeros((128 - ctx_tokens, 128), f32)], axis=0)
    gates_t = ctx_gates.T
    for item in range(items):
        head, d = item // 2, item % 2
        ctx_send[item] = jnp.concatenate(
            [
                gates_t[span * d + head : span * d + head + 1],
                gates_t[span * (2 + d) + head : span * (2 + d) + head + 1],
                jnp.zeros((6, 128), f32),
            ],
            axis=0,
        )
    for proj in projs[2:4]:
        proj.wait()
    project(tokens, ctx_tokens, 0, k_s, 0)
    project(tokens, ctx_tokens, 1, v_s, 0)

    def ctx_copies(item, place, slot, device):
        lanes = pl.ds((item // 2) * HEAD_DIM, HEAD_DIM)
        at = pl.ds(tokens, ctx_tokens)
        pairs = [
            (k_s.at[at, lanes], ctx_k.at[slot, place]),
            (v_s.at[at, lanes], ctx_v.at[slot, place]),
            (ctx_send.at[item], ctx_g.at[slot, place]),
        ]
        return [
            send(src, dst, sent_c.at[item, j], recv_c.at[slot, place, j], device) for j, (src, dst) in enumerate(pairs)
        ]

    for item in range(items):
        owner, slot = item // per, item % per

        @pl.when(owner != me)
        def _():
            for copy in ctx_copies(item, me, slot, on_mesh(sp=owner)):
                copy.start()

        @pl.when(owner == me)
        def _():
            lanes = slice((item // 2) * HEAD_DIM, (item // 2 + 1) * HEAD_DIM)
            ctx_k[slot, me] = k_s[tokens : tokens + ctx_tokens, lanes]
            ctx_v[slot, me] = v_s[tokens : tokens + ctx_tokens, lanes]
            ctx_g[slot, me] = ctx_send[item]

    modulate_rows(0, tokens, 0)
    size = min(CHUNK, tokens)
    gates = make_gates(0, tokens, size)
    for at in range(0, tokens, 128):
        block_t = gates[at : at + 128].T
        for head in range(heads):
            rows_g[head, :, at : at + 128] = jnp.concatenate(
                [
                    block_t[base + head : base + head + 1] for base in range(0, 4 * span, span)
                ]
                + [jnp.zeros((4, 128), f32)],
                axis=0,
            )
    project(0, tokens, 0, k_s, 0)
    project(0, tokens, 1, v_s, 0)
    projs[4].wait()
    project(0, tokens, 2, q_s, 0)

    blocks_here = sp // 2
    one_way = lax.rem(me + 1, 2)
    other_way = 1 - one_way

    def lanes_of(head):
        return pl.ds(pl.multiple_of(head * HEAD_DIM, HEAD_DIM), HEAD_DIM)

    def map_copy(head, towards):
        d = other_way
        return send(
            maps.at[head, d], got_map.at[head], sent_m.at[head], recv_m.at[head], on_mesh(sp=me + towards)
        )

    out_step = 1 - 2 * other_way
    in_step = 1 - 2 * one_way

    def stage_a(head):
        lanes = lanes_of(head)
        prepare_maps(
            tokens,
            span,
            k_s.at[:, lanes],
            v_s.at[:, lanes],
            cols.at[head],
            rows_g.at[head],
            srow.at[head],
            solved.at[head],
            carry.at[head],
            maps.at[head],
        )
        map_copy(head, out_step).start()

    def stage_b(head):
        lanes = lanes_of(head)
        prepare_outputs(
            tokens,
            span,
            q_s.at[:, lanes],
            k_s.at[:, lanes],
            cols.at[head],
            rows_g.at[head],
            srow.at[head],
            solved.at[head],
            carry.at[head],
            o_s.at[head],
            e_s.at[head],
        )

    def stage_pair(head):
        map_copy(head, -in_step).wait_recv()
        theirs, mine = got_map[head], maps[head, one_way]
        pair_map[head] = (
            theirs.astype(f32)
            + mine.astype(f32)
            + jnp.dot(mine[:, HEAD_DIM:], theirs, preferred_element_type=f32)
        )

    def first_devices(d):
        return [d * (sp - 1) + (1 - 2 * d) * i for i in range(2)]

    def zero_copy(slot, item, j):
        head, d = item // 2, lax.rem(item, 2)
        return first_devices(d)[j], send(
            s_zero.at[slot],
            start_in.at[head, d],
            sent_s.at[slot, j],
            recv_s.at[head, d],
            on_mesh(sp=first_devices(d)[j]),
        )

    def stage_context():
        for slot in range(per):
            item = me * per + slot

            @pl.when(item < items)
            def _():
                for r in range(1, sp):
                    src = lax.rem(me + r, sp)
                    for j, spot in enumerate((ctx_k.at[slot, src], ctx_v.at[slot, src], ctx_g.at[slot, src])):
                        send(spot, spot, sent_c.at[0, j], recv_c.at[slot, src, j], on_mesh(sp=src)).wait_recv()
                state = context_state(sp, lax.rem(item, 2), ctx_k.at[slot], ctx_v.at[slot], ctx_g.at[slot])
                s_zero[slot] = state.astype(bf16)
                for j in range(2):
                    device, copy = zero_copy(slot, item, j)

                    @pl.when(device != me)
                    def _():
                        copy.start()

                    @pl.when(device == me)
                    def _():
                        start_in[item // 2, lax.rem(item, 2)] = state.astype(bf16)

    def rank_block(d):
        return (d * (sp - 1) + (1 - 2 * d) * me) // 2

    def hop_copy(head, j):
        d = one_way
        return send(
            hop_out.at[head],
            start_in.at[head, d],
            sent_h.at[head, j],
            recv_s.at[head, d],
            on_mesh(sp=me + in_step * (2 - j)),
        )

    def stage_state(head, d):
        block = rank_block(d)
        owner = (2 * head + d) // per

        @pl.when((block > 0) | (owner != me))
        def _():
            spot = start_in.at[head, d]
            send(spot, spot, sent_h.at[head, 0], recv_s.at[head, d], on_mesh(sp=lax.rem(me + 1, sp))).wait_recv()

        state = start_in[head, d]

        @pl.when(d == one_way)
        def _():
            @pl.when(block < blocks_here - 1)
            def _():
                pair = pair_map[head]
                hop_out[head] = (
                    state.astype(f32)
                    + pair[:, :HEAD_DIM]
                    + jnp.dot(pair[:, HEAD_DIM:].astype(bf16), state, preferred_element_type=f32)
                ).astype(bf16)
                for j in range(2):
                    hop_copy(head, j).start()

            theirs = got_map[head]
            start_own[head, d] = (
                state.astype(f32)
                + theirs[:, :HEAD_DIM].astype(f32)
                + jnp.dot(theirs[:, HEAD_DIM:], state, preferred_element_type=f32)
            ).astype(bf16)

        @pl.when(d != one_way)
        def _():
            start_own[head, d] = state

    core = lax.rem(col, 2)
    partner = col + 1 - 2 * core
    chips = tp // 2
    far = [lax.rem(col + 2 * r, tp) for r in range(1, chips)]
    far_partner = [place + 1 - 2 * core for place in far]

    def far_copy(head, r):
        spot = ho.at[col, head]
        return send(spot, spot, sent_y.at[head, r], recv_y.at[head, col], on_mesh(tp=far[r]))

    def partner_copy(head):
        spot = ho.at[col, head]
        return send(spot, spot, sent_p.at[head], recv_p.at[head], on_mesh(tp=partner))

    def relay_copy(head, r):
        spot = ho.at[far[r], head]
        return send(spot, spot, sent_r.at[head, r], recv_r.at[head, far[r]], on_mesh(tp=partner))

    def stage_final(head):
        states = jnp.concatenate([start_own[head, 0], start_own[head, 1]], axis=0)
        combined = o_s[head] + jnp.dot(e_s[head], states, preferred_element_type=f32)
        scale = lax.rsqrt(jnp.mean(combined * combined, axis=1, keepdims=True) + epsilon)
        ho[col, head] = (combined * scale * head_gain_ref[...]).astype(bf16)
        for r in range(chips - 1):
            far_copy(head, r).start()
        partner_copy(head).start()

    first_dir = jnp.where(me < sp // 2, 0, 1)
    near_block = rank_block(first_dir)
    far_block = blocks_here - 1 - near_block

    def lag(block):
        return 1 + 2 * block + jnp.where(block >= 2, 1, 0)

    def slot_events(s):
        head1 = s - lag(near_block)

        @pl.when((head1 >= 0) & (head1 < heads))
        def _():
            stage_state(head1, first_dir)

        head2 = s - lag(far_block)

        @pl.when((head2 >= 0) & (head2 < heads))
        def _():
            stage_state(head2, 1 - first_dir)
            stage_final(head2)

    def loop_a(head, unused):
        stage_a(head)

        @pl.when(head == 0)
        def _():
            stage_context()

        @pl.when(head > 0)
        def _():
            stage_pair(head - 1)

        slot_events(head)
        return unused

    lax.fori_loop(0, heads, loop_a, 0)

    def loop_b(head, unused):
        stage_b(head)

        @pl.when(head == 0)
        def _():
            stage_pair(heads - 1)

        slot_events(heads + head)
        return unused

    lax.fori_loop(0, heads, loop_b, 0)
    last_slot = heads + 1 + 2 * (blocks_here - 1) + (1 if blocks_here > 2 else 0)

    def loop_c(s, unused):
        slot_events(s)
        return unused

    lax.fori_loop(2 * heads, last_slot, loop_c, 0)
    out_load.wait()
    group = min(2, heads)

    def add(src, first, count, start):
        block = jnp.concatenate([ho[src, first + i] for i in range(count)], axis=1)

        def columns(j, unused):
            lanes = pl.ds(pl.multiple_of(j * tile, tile), tile)
            at = pl.ds(pl.multiple_of(src * out_width + first * HEAD_DIM, HEAD_DIM), count * HEAD_DIM)
            part = jnp.dot(block, wo[at, lanes], preferred_element_type=f32)
            acc[:, lanes] = part if start else acc[:, lanes] + part
            return unused

        lax.fori_loop(0, width // tile, columns, 0)

    add(col, 0, heads, True)
    for head in range(heads):
        spot = ho.at[partner, head]
        send(spot, spot, sent_p.at[head], recv_p.at[head], on_mesh(tp=partner)).wait_recv()
    add(partner, 0, heads, False)
    for first in range(0, heads, group):
        for head in range(first, first + group):
            for r, src in enumerate(far):
                spot = ho.at[src, head]
                send(spot, spot, sent_y.at[head, r], recv_y.at[head, src], on_mesh(tp=src)).wait_recv()
                relay_copy(head, r).start()
        for src in far:
            add(src, first, group, False)
        for head in range(first, first + group):
            for r, src in enumerate(far_partner):
                spot = ho.at[src, head]
                send(spot, spot, sent_r.at[head, r], recv_r.at[head, src], on_mesh(tp=partner)).wait_recv()
        for src in far_partner:
            add(src, first, group, False)

    def finish(i, unused):
        at = pl.ds(pl.multiple_of(i * step, step), step)
        residual = rows_in[at, pl.ds(pl.multiple_of(col * width, width), width)].astype(f32)
        out_ref[at, :] = (residual + gate_row[...] * acc[at, :]).astype(bf16)
        return unused

    lax.fori_loop(0, tokens // step, finish, 0)
    for copy in out:
        copy.wait_send()
    for item in range(items):
        owner, slot = item // per, item % per

        @pl.when(owner != me)
        def _():
            for copy in ctx_copies(item, me, slot, on_mesh(sp=owner)):
                copy.wait_send()

    for slot in range(per):
        item = me * per + slot

        @pl.when(item < items)
        def _():
            for j in range(2):
                device, copy = zero_copy(slot, item, j)

                @pl.when(device != me)
                def _():
                    copy.wait_send()

    for head in range(heads):
        map_copy(head, out_step).wait_send()

        @pl.when(rank_block(one_way) < blocks_here - 1)
        def _():
            for j in range(2):
                hop_copy(head, j).wait_send()

        for r in range(chips - 1):
            far_copy(head, r).wait_send()
            relay_copy(head, r).wait_send()
        partner_copy(head).wait_send()


def body(
    latent,
    context,
    condition,
    context_condition,
    shift_weight,
    scale_weight,
    gate_weight,
    norm_gain,
    query_weight,
    key_weight,
    value_weight,
    write_weight,
    decay_weight,
    write_bias,
    decay_bias,
    log_rate,
    head_gain,
    out_weight,
):
    sp, tp = lax.axis_size("sp"), lax.axis_size("tp")
    tokens, depth = latent.shape
    ctx_tokens = context.shape[0]
    rows = tokens + ctx_tokens
    out_width = query_weight.shape[1]
    heads = out_width // HEAD_DIM
    items = 2 * heads
    per = -(-items // sp)
    width = out_weight.shape[1]
    chunks = tokens // min(CHUNK, tokens)
    gate_rows = 2 * write_bias.shape[1]
    vmem = pl.BlockSpec(memory_space=pltpu.VMEM)
    anywhere = pl.BlockSpec(memory_space=pl.ANY)
    dma = pltpu.SemaphoreType.DMA
    square, wide = (HEAD_DIM, HEAD_DIM), (HEAD_DIM, 2 * HEAD_DIM)
    scratch = [
        ((3,) + shift_weight.shape, bf16),
        ((rows, depth), bf16),
        ((depth, 3 * out_width), bf16),
        ((2 * gate_rows, depth), bf16),
        (out_weight.shape, bf16),
        ((rows, 128), f32),
        ((rows, depth), bf16),
        ((tokens, out_width), bf16),
        ((rows, out_width), bf16),
        ((rows, out_width), bf16),
        ((sp, 8, width), bf16),
        ((tp, 4, width), f32),
        ((1, width), f32),
        ((heads, rows, 128), f32),
        ((heads, 8, tokens), f32),
        ((heads, 1, tokens), f32),
        ((heads, chunks, 2, tokens // chunks, 2 * HEAD_DIM), bf16),
        ((heads, chunks, 2) + wide, bf16),
        ((heads, 2) + wide, bf16),
        ((heads, tokens, HEAD_DIM), f32),
        ((heads, tokens, 2 * HEAD_DIM), bf16),
        ((items, 8, 128), f32),
        ((per, sp, ctx_tokens, HEAD_DIM), bf16),
        ((per, sp, ctx_tokens, HEAD_DIM), bf16),
        ((per, sp, 8, 128), f32),
        ((per,) + square, bf16),
        ((heads,) + wide, bf16),
        ((heads,) + wide, f32),
        ((heads, 2) + square, bf16),
        ((heads, 2) + square, bf16),
        ((heads,) + square, bf16),
        ((tp, heads, tokens, HEAD_DIM), bf16),
        ((tokens, width), f32),
    ]
    semaphores = [
        (11,), (sp,), (sp,), (tp,), (tp,), (items, 3), (per, sp, 3), (per, 2), (heads, 2), (heads,), (heads,),
        (heads, 2), (heads, tp), (heads, tp), (heads,), (heads,), (heads, tp), (heads, tp),
    ]
    return pl.pallas_call(
        functools.partial(mixer_kernel, sp, tp, heads, per),
        in_specs=[vmem] * 7 + [anywhere] * 11,
        out_specs=vmem,
        out_shape=jax.ShapeDtypeStruct((tokens, width), bf16),
        scratch_shapes=[pltpu.VMEM(shape, dtype) for shape, dtype in scratch] + [dma(shape) for shape in semaphores],
        compiler_params=pltpu.CompilerParams(
            collective_id=0, has_side_effects=True, vmem_limit_bytes=63 * 1024 * 1024
        ),
        name="mixer",
    )(
        condition.reshape(-1, 128),
        context_condition.reshape(-1, 128),
        norm_gain[None, :],
        head_gain[None, :],
        write_bias,
        decay_bias,
        log_rate,
        shift_weight,
        scale_weight,
        gate_weight,
        latent,
        context,
        jnp.transpose(write_weight, (1, 2, 0)).reshape(gate_rows, depth),
        jnp.transpose(decay_weight, (1, 2, 0)).reshape(gate_rows, depth),
        query_weight,
        key_weight,
        value_weight,
        out_weight,
    )


def solution(mesh):
    placed = (
        P("sp", None),
        P("sp", None),
        P("sp"),
        P("sp"),
        P("sp", "tp"),
        P("sp", "tp"),
        P("sp", "tp"),
        P(),
        P(None, "tp"),
        P(None, "tp"),
        P(None, "tp"),
        P(),
        P(),
        P(),
        P(),
        P(),
        P(),
        P(None, "tp"),
    )
    return jax.shard_map(body, mesh=mesh, in_specs=placed, out_specs=P("sp", "tp"), check_vma=False)
```

```python
import functools

import jax
import jax.numpy as jnp
from jax import lax
from jax.experimental import pallas as pl
from jax.experimental.pallas import tpu as pltpu
from jax.sharding import PartitionSpec as P

HEAD_DIM = 128
CHUNK = 128
epsilon = 0.0001
bf16 = jnp.bfloat16
f32 = jnp.float32


def mm(a, b):
    return jnp.dot(a.astype(bf16), b.astype(bf16), preferred_element_type=f32)


def on_mesh(sp=None, tp=None):
    return (lax.axis_index("sp") if sp is None else sp, lax.axis_index("tp") if tp is None else tp)


def send(src, dst, send_sem, recv_sem, device):
    return pltpu.make_async_remote_copy(
        src_ref=src,
        dst_ref=dst,
        send_sem=send_sem,
        recv_sem=recv_sem,
        device_id=device,
        device_id_type=pl.DeviceIdType.MESH,
    )


def greet(devices):
    barrier = pltpu.get_barrier_semaphore()
    for device in devices:
        pl.semaphore_signal(barrier, inc=1, device_id=device, device_id_type=pl.DeviceIdType.MESH)


def grid_iota(size):
    return (
        lax.broadcasted_iota(jnp.int32, (size, size), 0),
        lax.broadcasted_iota(jnp.int32, (size, size), 1),
    )


def bits(mask):
    return mask.astype(f32).astype(bf16)


def half_masks(size):
    half = size // 2
    lanes = lax.broadcasted_iota(jnp.int32, (half, size), 1)
    return bits(lanes < half), bits(lanes >= half)


def spread(compact, masks):
    return jnp.concatenate([compact * masks[0], compact * masks[1]], axis=0)


def invert_halves(items):
    for item in items:
        size = item["system"].shape[0]
        half = size // 2
        item["masks"] = half_masks(size)
        item["system"] = item["system"].astype(bf16)
        item["pieces"] = item["system"][:half] * item["masks"][0] + item["system"][half:] * item["masks"][1]
        rows = lax.broadcasted_iota(jnp.int32, (half, size), 0)
        cols = lax.rem(lax.broadcasted_iota(jnp.int32, (half, size), 1), half)
        item["grid"] = (rows, cols)
        item["inv"] = bits(rows == cols) - item["pieces"] * bits((rows // 2) == (cols // 2))
    step = 2
    while step < max(item["inv"].shape[0] for item in items):
        firsts = []
        active = [item for item in items if step < item["inv"].shape[0]]
        for item in active:
            rows, cols = item["grid"]
            late, early = item["order"](rows, cols)
            late, early = late // step, early // step
            mask = bits(((late % 2) == 1) & (early == late - 1))
            firsts.append(mm(item["pieces"] * mask, spread(item["inv"], item["masks"])).astype(bf16))
        for item, first in zip(active, firsts):
            item["inv"] = item["inv"] - mm(item["inv"], spread(first, item["masks"])).astype(bf16)
        step *= 2


def solve_halves(items):
    def halves(item):
        half = item["inv"].shape[0]
        first, second = item["masks"]
        return half, first, second

    for item in items:
        half, first, second = halves(item)
        both = item["both"].astype(bf16)
        lead = item["pick"](first, second)
        item["lead"] = mm(item["inv"] * lead, both).astype(bf16)
    for item in items:
        half, first, second = halves(item)
        lead = item["lead"]
        mix = item["pick"](item["system"][half:] * first, item["system"][:half] * second)
        item["rest"] = item["pick"](item["both"][half:], item["both"][:half]) - mm(
            mix, jnp.concatenate([lead, lead], axis=0)
        )
    for item in items:
        half, first, second = halves(item)
        rest = item["rest"].astype(bf16)
        trail = mm(
            item["inv"] * item["pick"](second, first), jnp.concatenate([rest, rest], axis=0)
        ).astype(bf16)
        lead = item["lead"]
        item["solved"] = jnp.concatenate([item["pick"](lead, trail), item["pick"](trail, lead)], axis=0)


def chooser(d):
    if isinstance(d, int):
        return lambda a, b: a if d == 0 else b
    return lambda a, b: jnp.where(d == 0, a, b)


def orderer(d):
    if isinstance(d, int):
        return lambda a, b: (a, b) if d == 0 else (b, a)
    return lambda a, b: (jnp.where(d == 0, a, b), jnp.where(d == 0, b, a))


def key_grams(keys):
    size = keys.shape[0]
    rows, cols = grid_iota(size)
    keys_t = keys.astype(f32).T
    gram = jnp.dot(keys, keys_t.astype(bf16), preferred_element_type=f32)
    diag = jnp.where(rows == cols, gram, 0.0)
    s_col = lax.rsqrt(jnp.sum(diag, axis=1, keepdims=True) + epsilon)
    s_row = lax.rsqrt(jnp.sum(diag, axis=0, keepdims=True) + epsilon)
    return gram * s_col * s_row, keys.astype(f32) * s_col, keys_t * s_row, s_row


def eye_matrix():
    rows, cols = grid_iota(HEAD_DIM)
    return (rows == cols).astype(f32)


def make_item(d, gram, keys, keys_t, values, rate_col, run_col, run_row):
    rows, cols = grid_iota(gram.shape[0])
    order = orderer(d)
    late, early = order(rows, cols)
    decay = jnp.where(late > early, jnp.exp(jnp.minimum(run_col - run_row, 0.0)), 0.0)
    both = jnp.concatenate([values * rate_col, keys * (rate_col * jnp.exp(run_col))], axis=1)
    size = gram.shape[0]
    last = chooser(d)(run_row[:, size - 1 :], run_row[:, :1])
    return dict(
        order=order,
        pick=chooser(d),
        system=gram * decay * rate_col,
        both=both,
        gate=jnp.exp(last),
        late_t=(keys_t * jnp.exp(last - run_row)).astype(bf16),
    )


def latent_items(tokens, span, refs):
    size = min(CHUNK, tokens)
    k_ref, v_ref, col_ref, row_ref, srow_ref = refs[:5]
    items = []
    for at in range(0, tokens, size):
        gram, keys, keys_t, s_row = key_grams(k_ref[at : at + size, :])
        srow_ref[:, at : at + size] = s_row
        values = v_ref[at : at + size, :].astype(f32)
        for d in range(2):
            rate_col = col_ref[at : at + size, span * d : span * d + 1]
            run_col = col_ref[at : at + size, span * (2 + d) : span * (2 + d) + 1]
            run_row = row_ref[2 + d : 3 + d, at : at + size]
            item = make_item(d, gram, keys, keys_t, values, rate_col, run_col, run_row)
            item["d"], item["index"] = d, at // size
            items.append(item)
    return items


def context_items(places, d, k_ref, v_ref, g_ref):
    size = k_ref.shape[1]
    items = []
    for step in range(places):
        place = step + d * (places - 1 - 2 * step)
        gram, keys, keys_t, unused = key_grams(k_ref[place])
        gates = g_ref[place]
        gates_t = gates.T
        items.append(
            make_item(
                d, gram, keys, keys_t, v_ref[place].astype(f32),
                gates_t[:size, 0:1], gates_t[:size, 1:2], gates[1:2, :size],
            )
        )
    return items


def solve_items(items):
    invert_halves(items)
    solve_halves(items)
    for item in items:
        item["late"] = mm(item["late_t"], item["solved"])


def latent_maps(groups):
    eye = eye_matrix()
    chains = []
    for items, refs in groups:
        solved_ref, carry_ref, map_ref = refs[5:]
        for item in items:
            solved_ref[item["index"], item["d"]] = item["solved"]
        for d in range(2):
            chain = [i for i in items if i["d"] == d]
            chains.append((chain if d == 0 else chain[::-1], d, carry_ref, map_ref))
    carries = [None] * len(chains)
    for position in range(len(chains[0][0])):
        for which, (chain, d, carry_ref, map_ref) in enumerate(chains):
            item = chain[position]
            late, gate = item["late"], item["gate"]
            fresh = jnp.concatenate([late[:, :HEAD_DIM], (gate - 1.0) * eye - late[:, HEAD_DIM:]], axis=1)
            if position == 0:
                carries[which] = fresh
            else:
                held = carries[which].astype(bf16)
                carry_ref[item["index"], d] = held
                carries[which] = gate * carries[which] + fresh - mm(late[:, HEAD_DIM:], held)
    for carry, (chain, d, carry_ref, map_ref) in zip(carries, chains):
        map_ref[d] = carry.astype(bf16)


def context_state(items):
    state = items[0]["late"][:, :HEAD_DIM]
    for item in items[1:]:
        late = item["late"]
        state = item["gate"] * state + late[:, :HEAD_DIM] - mm(late[:, HEAD_DIM:], state)
    return state.astype(bf16)


def prepare_outputs(tokens, span, q_ref, k_ref, col_ref, row_ref, srow_ref, solved_ref, carry_ref, o_ref, e_ref):
    size = min(CHUNK, tokens)
    rows, cols = grid_iota(size)
    count = tokens // size
    for index in range(count):
        at = index * size
        raw = q_ref[at : at + size, :]
        queries = raw.astype(f32)
        q_scale = lax.rsqrt(jnp.sum(queries * queries, axis=1, keepdims=True) + epsilon) * HEAD_DIM**-0.5
        queries = queries * q_scale
        score = lax.dot_general(
            raw, k_ref[at : at + size, :], (((1,), (1,)), ((), ())), preferred_element_type=f32
        ) * (q_scale * srow_ref[:, at : at + size])
        total = None
        for d in range(2):
            run_col = col_ref[at : at + size, span * (2 + d) : span * (2 + d) + 1]
            run_row = row_ref[2 + d : 3 + d, at : at + size]
            inside = rows >= cols if d == 0 else rows <= cols
            decay = jnp.where(inside, jnp.exp(jnp.minimum(run_col - run_row, 0.0)), 0.0)
            weighed = mm(score * decay, solved_ref[index, d])
            local = weighed[:, :HEAD_DIM]
            early = queries * jnp.exp(run_col) - weighed[:, HEAD_DIM:]
            if index != (0 if d == 0 else count - 1):
                moved = mm(early, carry_ref[index, d])
                local = local + moved[:, :HEAD_DIM]
                early = early + moved[:, HEAD_DIM:]
            e_ref[at : at + size, d * HEAD_DIM : (d + 1) * HEAD_DIM] = early.astype(bf16)
            total = local if total is None else total + local
        o_ref[at : at + size, :] = total


def log1p_unit(u):
    z = u / (2.0 + u)
    z2 = z * z
    series = 1.0 / 11.0 + 0.0 * z2
    for power in (9, 7, 5, 3, 1):
        series = series * z2 + 1.0 / power
    return 2.0 * z * series


def triangle_sums(lower, parts):
    return sum(jnp.dot(lower, part, preferred_element_type=f32) for part in parts)


def split_three(values):
    high = values.astype(bf16)
    rest = values - high.astype(f32)
    middle = rest.astype(bf16)
    return high, middle, (rest - middle.astype(f32)).astype(bf16)


def mixer_kernel(
    sp, tp, heads, per,
    cond_ref, ctx_cond_ref, gain_ref, head_gain_ref, wb_ref, db_ref, lr_ref,
    shift_ref, scale_ref, gate_ref, latent_ref, context_ref, write_ref, decay_ref,
    wq_ref, wk_ref, wv_ref, wo_ref,
    out_ref,
    mod_w, rows_in, weights, gate_w, wo, rstd, mixed, q_s, k_s, v_s,
    got, blocks, gate_row, cols, rows_g, srow, solved, carry, maps, o_s, e_s,
    ctx_send, ctx_k, ctx_v, ctx_g, s_zero, got_map, pair_map, start_in, start_own, hop_out, ho, acc,
    local_sems, sent_a, recv_a, sent_b, recv_b, sent_c, recv_c, sent_s, recv_s, sent_m, recv_m,
    sent_h, sent_y, recv_y, sent_p, recv_p, sent_r, recv_r,
):
    me, col = lax.axis_index("sp"), lax.axis_index("tp")
    width = shift_ref.shape[1]
    tokens, ctx_tokens = latent_ref.shape[0], context_ref.shape[0]
    total_rows = tokens + ctx_tokens
    depth = latent_ref.shape[1]
    out_width = heads * HEAD_DIM
    items = 2 * heads
    loads = []

    def load(src, dst):
        loads.append(pltpu.make_async_copy(src, dst, local_sems.at[len(loads)]))
        loads[-1].start()
        return loads[-1]

    mods = [load(ref, mod_w.at[i]) for i, ref in enumerate([shift_ref, scale_ref, gate_ref])]
    acts = [
        load(context_ref, rows_in.at[pl.ds(tokens, ctx_tokens)]),
        load(latent_ref, rows_in.at[pl.ds(0, tokens)]),
    ]
    gate_rows = write_ref.shape[0]
    projs = [
        load(write_ref, gate_w.at[pl.ds(0, gate_rows)]),
        load(decay_ref, gate_w.at[pl.ds(gate_rows, gate_rows)]),
    ]
    projs += [
        load(ref, weights.at[:, pl.ds(i * out_width, out_width)]) for i, ref in enumerate([wk_ref, wv_ref, wq_ref])
    ]
    out_load = load(wo_ref, wo)
    rings = [on_mesh(sp=lax.rem(me + r, sp)) for r in range(1, sp)]
    cross = [on_mesh(tp=lax.rem(col + r, tp)) for r in range(1, tp)]
    greet(rings + cross)

    def flat(ref):
        values = ref[...].astype(f32)
        return jnp.concatenate([values[i : i + 1] for i in range(values.shape[0])], axis=1)

    silu = jnp.concatenate([flat(cond_ref), flat(ctx_cond_ref), jnp.zeros((6, cond_ref.size), f32)], axis=0)
    silu = (silu / (1.0 + jnp.exp(-silu))).astype(bf16)
    parts = []
    for i in range(3):
        mods[i].wait()
        parts.append(jnp.dot(silu, mod_w[i], preferred_element_type=f32))
    got[me] = jnp.concatenate(
        [parts[0][0:2], parts[1][0:2], parts[2][0:1], jnp.zeros((3, width), f32)], axis=0
    ).astype(bf16)
    pl.semaphore_wait(pltpu.get_barrier_semaphore(), len(rings) + len(cross))
    out = []
    for r, device in enumerate(rings):
        out.append(send(got.at[me], got.at[me], sent_a.at[r], recv_a.at[me], device))
        out[-1].start()
    for act in acts:
        act.wait()
    step = 16

    def stats(i, unused):
        at = pl.ds(pl.multiple_of(i * step, step), step)
        values = rows_in[at, :].astype(f32)
        mean = jnp.sum(values * values, axis=1, keepdims=True) * (1.0 / depth)
        rstd[at, :] = jnp.broadcast_to(lax.rsqrt(mean + epsilon), (step, 128))
        return unused

    lax.fori_loop(0, total_rows // step, stats, 0)
    for r in range(1, sp):
        src = lax.rem(me + r, sp)
        send(got.at[src], got.at[src], sent_a.at[0], recv_a.at[src], on_mesh(sp=src)).wait_recv()
    summed = got[0].astype(f32)
    for place in range(1, sp):
        summed = summed + got[place].astype(f32)
    blocks[col] = summed[0:4]
    gate_row[...] = summed[4:5]
    for r, device in enumerate(cross):
        out.append(send(blocks.at[col], blocks.at[col], sent_b.at[r], recv_b.at[col], device))
        out[-1].start()
    core = lax.rem(col, 2)
    partner = col + 1 - 2 * core
    chips = tp // 2
    far = [lax.rem(col + 2 * r, tp) for r in range(1, chips)]
    far_partner = [place + 1 - 2 * core for place in far]

    def block_arrive(src):
        send(blocks.at[src], blocks.at[src], sent_b.at[0], recv_b.at[src], on_mesh(tp=src)).wait_recv()

    def modulate_rows(place, start, count, index):
        lanes = pl.ds(pl.multiple_of(place * width, width), width)
        block = blocks[place]
        slope = gain_ref[:, lanes] * (1.0 + block[2 + index : 3 + index])
        shift = block[index : index + 1]

        def modulate(i, unused):
            at = pl.ds(pl.multiple_of(start + i * step, step), step)
            scale = jnp.concatenate([rstd[at, :]] * (width // 128), axis=1)
            mixed[at, lanes] = (rows_in[at, lanes].astype(f32) * scale * slope + shift).astype(bf16)
            return unused

        lax.fori_loop(0, count // step, modulate, 0)

    modulate_rows(col, tokens, ctx_tokens, 1)
    modulate_rows(col, 0, tokens, 0)
    block_arrive(partner)
    modulate_rows(partner, tokens, ctx_tokens, 1)
    modulate_rows(partner, 0, tokens, 0)
    for place in far + far_partner:
        block_arrive(place)
        modulate_rows(place, tokens, ctx_tokens, 1)

    tile = 256 if out_width % 256 == 0 else 128

    def project(first, count, which, ref, base):
        def columns(j, unused):
            lanes = pl.ds(pl.multiple_of(which * out_width + j * tile, tile), tile)
            part = jnp.dot(mixed[pl.ds(first, count), :], weights[:, lanes], preferred_element_type=f32)
            ref[pl.ds(first, count), pl.ds(pl.multiple_of(j * tile, tile), tile)] = part.astype(bf16)
            return unused

        lax.fori_loop(0, out_width // tile, columns, 0)

    first_head = col * heads
    span = wb_ref.shape[1]
    bias = jnp.concatenate([wb_ref[0:1], wb_ref[1:2], db_ref[0:1], db_ref[1:2]], axis=1)
    rates = jnp.concatenate([lr_ref[0:1], lr_ref[1:2]] * 2, axis=1)
    lanes_here = bias.shape[1]

    def make_gates(first, count, size):
        pre = lax.dot_general(
            mixed[pl.ds(first, count), :], gate_w[...], (((1,), (1,)), ((), ())), preferred_element_type=f32
        ).astype(bf16).astype(f32) + bias
        rate = 1.0 / (1.0 + jnp.exp(-pre))
        decay = -jnp.exp(rates) * (jnp.maximum(pre, 0.0) + log1p_unit(jnp.exp(-jnp.abs(pre))))
        lane = lax.broadcasted_iota(jnp.int32, (count, lanes_here), 1)
        rows, columns = grid_iota(size)
        lower, upper = (rows >= columns).astype(bf16), (rows <= columns).astype(bf16)
        backward = lax.broadcasted_iota(jnp.int32, (size, lanes_here), 1) >= 3 * span
        running = []
        for at in range(0, count, size):
            split = split_three(decay[at : at + size])
            running.append(jnp.where(backward, triangle_sums(upper, split), triangle_sums(lower, split)))
        gates = jnp.where(lane < 2 * span, rate, jnp.concatenate(running, axis=0))
        gates = jnp.concatenate([gates, jnp.zeros((count, 128 - lanes_here), f32)], axis=1)
        gates = pltpu.roll(gates, lax.rem(128 - first_head, 128), 1)
        for head in range(heads):
            cols[head, pl.ds(first, count), :] = gates if head == 0 else pltpu.roll(gates, 128 - head, 1)
        return gates

    for proj in projs[:2]:
        proj.wait()
    ctx_gates = make_gates(tokens, ctx_tokens, ctx_tokens)
    if ctx_tokens < 128:
        ctx_gates = jnp.concatenate([ctx_gates, jnp.zeros((128 - ctx_tokens, 128), f32)], axis=0)
    gates_t = ctx_gates.T
    for item in range(items):
        head, d = item // 2, item % 2
        ctx_send[item] = jnp.concatenate(
            [
                gates_t[span * d + head : span * d + head + 1],
                gates_t[span * (2 + d) + head : span * (2 + d) + head + 1],
                jnp.zeros((6, 128), f32),
            ],
            axis=0,
        )
    for proj in projs[2:4]:
        proj.wait()
    project(tokens, ctx_tokens, 0, k_s, 0)
    project(tokens, ctx_tokens, 1, v_s, 0)

    def ctx_copies(item, place, slot, device):
        lanes = pl.ds((item // 2) * HEAD_DIM, HEAD_DIM)
        at = pl.ds(tokens, ctx_tokens)
        pairs = [
            (k_s.at[at, lanes], ctx_k.at[slot, place]),
            (v_s.at[at, lanes], ctx_v.at[slot, place]),
            (ctx_send.at[item], ctx_g.at[slot, place]),
        ]
        return [
            send(src, dst, sent_c.at[item, j], recv_c.at[slot, place, j], device) for j, (src, dst) in enumerate(pairs)
        ]

    for item in range(items):
        owner, slot = item // per, item % per

        @pl.when(owner != me)
        def _():
            for copy in ctx_copies(item, me, slot, on_mesh(sp=owner)):
                copy.start()

        @pl.when(owner == me)
        def _():
            lanes = slice((item // 2) * HEAD_DIM, (item // 2 + 1) * HEAD_DIM)
            ctx_k[slot, me] = k_s[tokens : tokens + ctx_tokens, lanes]
            ctx_v[slot, me] = v_s[tokens : tokens + ctx_tokens, lanes]
            ctx_g[slot, me] = ctx_send[item]

    for place in far + far_partner:
        modulate_rows(place, 0, tokens, 0)
    size = min(CHUNK, tokens)
    gates = make_gates(0, tokens, size)
    for j in range(out_width // tile):
        lanes = slice(j * tile, (j + 1) * tile)
        k_s[0:tokens, lanes] = jnp.dot(mixed[0:tokens, :], weights[:, lanes], preferred_element_type=f32).astype(bf16)
    for at in range(0, tokens, 128):
        block_t = gates[at : at + 128].T
        for head in range(heads):
            rows_g[head, :, at : at + 128] = jnp.concatenate(
                [
                    block_t[base + head : base + head + 1] for base in range(0, 4 * span, span)
                ]
                + [jnp.zeros((4, 128), f32)],
                axis=0,
            )
    project(0, tokens, 1, v_s, 0)

    blocks_here = sp // 2
    one_way = lax.rem(me + 1, 2)
    other_way = 1 - one_way

    def lanes_of(head):
        return pl.ds(pl.multiple_of(head * HEAD_DIM, HEAD_DIM), HEAD_DIM)

    def map_copy(head, towards):
        d = other_way
        return send(
            maps.at[head, d], got_map.at[head], sent_m.at[head], recv_m.at[head], on_mesh(sp=me + towards)
        )

    out_step = 1 - 2 * other_way
    in_step = 1 - 2 * one_way

    def refs_of(head):
        lanes = lanes_of(head)
        return (
            k_s.at[:, lanes], v_s.at[:, lanes], cols.at[head], rows_g.at[head], srow.at[head],
            solved.at[head], carry.at[head], maps.at[head],
        )

    def stage_a(members, extra=()):
        groups = [(latent_items(tokens, span, refs_of(head)), refs_of(head)) for head in members]
        solve_items([item for group, unused in groups for item in group] + list(extra))
        latent_maps(groups)
        for head in members:
            map_copy(head, out_step).start()

    def stage_b(members):
        for head in members:
            lanes = lanes_of(head)
            prepare_outputs(
                tokens,
                span,
                q_s.at[:, lanes],
                k_s.at[:, lanes],
                cols.at[head],
                rows_g.at[head],
                srow.at[head],
                solved.at[head],
                carry.at[head],
                o_s.at[head],
                e_s.at[head],
            )

    def stage_pair(members):
        for head in members:
            map_copy(head, -in_step).wait_recv()
        for head in members:
            theirs, mine = got_map[head], maps[head, one_way]
            pair_map[head] = (
                theirs.astype(f32)
                + mine.astype(f32)
                + jnp.dot(mine[:, HEAD_DIM:], theirs, preferred_element_type=f32)
            )

    def first_devices(d):
        return [d * (sp - 1) + (1 - 2 * d) * i for i in range(2)]

    def zero_copy(slot, item, j):
        head, d = item // 2, lax.rem(item, 2)
        return first_devices(d)[j], send(
            s_zero.at[slot],
            start_in.at[head, d],
            sent_s.at[slot, j],
            recv_s.at[head, d],
            on_mesh(sp=first_devices(d)[j]),
        )

    def context_wait(slot):
        for r in range(1, sp):
            src = lax.rem(me + r, sp)
            for j, spot in enumerate((ctx_k.at[slot, src], ctx_v.at[slot, src], ctx_g.at[slot, src])):
                send(spot, spot, sent_c.at[0, j], recv_c.at[slot, src, j], on_mesh(sp=src)).wait_recv()

    def context_parts(slot, item):
        return context_items(sp, lax.rem(item, 2), ctx_k.at[slot], ctx_v.at[slot], ctx_g.at[slot])

    def context_ship(slot, item, state):
        s_zero[slot] = state
        for j in range(2):
            device, copy = zero_copy(slot, item, j)

            @pl.when(device != me)
            def _():
                copy.start()

            @pl.when(device == me)
            def _():
                start_in[item // 2, lax.rem(item, 2)] = state

    def rank_block(d):
        return (d * (sp - 1) + (1 - 2 * d) * me) // 2

    def hop_copy(head, j):
        d = one_way
        return send(
            hop_out.at[head],
            start_in.at[head, d],
            sent_h.at[head, j],
            recv_s.at[head, d],
            on_mesh(sp=me + in_step * (2 - j)),
        )

    def stage_state(members, d):
        block = rank_block(d)
        moving = (d == one_way) & (block < blocks_here - 1)
        for head in members:
            owner = (2 * head + d) // per

            @pl.when((block > 0) | (owner != me))
            def _():
                spot = start_in.at[head, d]
                send(spot, spot, sent_h.at[head, 0], recv_s.at[head, d], on_mesh(sp=lax.rem(me + 1, sp))).wait_recv()

            @pl.when(moving)
            def _():
                state = start_in[head, d]
                pair = pair_map[head]
                hop_out[head] = (
                    state.astype(f32)
                    + pair[:, :HEAD_DIM]
                    + jnp.dot(pair[:, HEAD_DIM:].astype(bf16), state, preferred_element_type=f32)
                ).astype(bf16)
                hop_copy(head, 0).start()

        @pl.when(moving)
        def _():
            for head in members:
                hop_copy(head, 1).start()

        @pl.when(d == one_way)
        def _():
            for head in members:
                state, theirs = start_in[head, d], got_map[head]
                start_own[head, d] = (
                    state.astype(f32)
                    + theirs[:, :HEAD_DIM].astype(f32)
                    + jnp.dot(theirs[:, HEAD_DIM:], state, preferred_element_type=f32)
                ).astype(bf16)

        @pl.when(d != one_way)
        def _():
            for head in members:
                start_own[head, d] = start_in[head, d]

    def far_copy(head, r):
        spot = ho.at[col, head]
        return send(spot, spot, sent_y.at[head, r], recv_y.at[head, col], on_mesh(tp=far[r]))

    def partner_copy(head):
        spot = ho.at[col, head]
        return send(spot, spot, sent_p.at[head], recv_p.at[head], on_mesh(tp=partner))

    def relay_copy(head, r):
        spot = ho.at[far[r], head]
        return send(spot, spot, sent_r.at[head, r], recv_r.at[head, far[r]], on_mesh(tp=partner))

    def stage_final(head):
        states = jnp.concatenate([start_own[head, 0], start_own[head, 1]], axis=0)
        combined = o_s[head] + jnp.dot(e_s[head], states, preferred_element_type=f32)
        scale = lax.rsqrt(jnp.mean(combined * combined, axis=1, keepdims=True) + epsilon)
        ho[col, head] = (combined * scale * head_gain_ref[...]).astype(bf16)
        for r in range(chips - 1):
            far_copy(head, r).start()
        partner_copy(head).start()

    first_dir = jnp.where(me < sp // 2, 0, 1)
    near_block = rank_block(first_dir)
    far_block = blocks_here - 1 - near_block

    def near_event(members):
        stage_state(members, first_dir)

    def far_event(members):
        stage_state(members, 1 - first_dir)
        for head in members:
            stage_final(head)

    team = 2 if heads % 2 == 0 else 1
    teams = [list(range(at, at + team)) for at in range(0, heads, team)]
    for index, members in enumerate(teams):
        if index == 0 and items == per * sp:
            for slot in range(per):
                context_wait(slot)
            extras = [context_parts(slot, me * per + slot) for slot in range(per)]
            stage_a(members, [item for extra in extras for item in extra])
            for slot, extra in enumerate(extras):
                context_ship(slot, me * per + slot, context_state(extra))
        elif index == 0:
            stage_a(members)
            for slot in range(per):
                item = me * per + slot

                @pl.when(item < items)
                def _():
                    context_wait(slot)
                    extra = context_parts(slot, item)
                    solve_items(extra)
                    context_ship(slot, item, context_state(extra))
        else:
            stage_a(members)
            stage_pair(teams[index - 1])

            @pl.when(near_block == 0)
            def _():
                near_event(teams[index - 1])

    projs[4].wait()
    project(0, tokens, 2, q_s, 0)
    stage_pair(teams[-1])

    @pl.when(near_block == 0)
    def _():
        near_event(teams[-1])

    @pl.when(near_block > 0)
    def _():
        near_event(teams[0])

    for members in teams:
        stage_b(members)

    @pl.when(near_block > 0)
    def _():
        for members in teams[1:]:
            near_event(members)

    for members in teams:
        far_event(members)
    out_load.wait()
    def multiply(spans, finish):
        def columns(j, unused):
            lanes = pl.ds(pl.multiple_of(j * tile, tile), tile)
            part = None
            for src, first, count in spans:
                block = jnp.concatenate([ho[src, first + i] for i in range(count)], axis=1)
                at = pl.ds(pl.multiple_of(src * out_width + first * HEAD_DIM, HEAD_DIM), count * HEAD_DIM)
                term = jnp.dot(block, wo[at, lanes], preferred_element_type=f32)
                part = term if part is None else part + term
            finish(j, lanes, part)
            return unused

        lax.fori_loop(0, width // tile, columns, 0)

    def first_part(j, lanes, part):
        acc[:, lanes] = part

    def middle_part(j, lanes, part):
        acc[:, lanes] = acc[:, lanes] + part

    def last_part(j, lanes, part):
        residual = rows_in[pl.ds(0, tokens), pl.ds(pl.multiple_of(col * width + j * tile, tile), tile)].astype(f32)
        out_ref[:, lanes] = (residual + gate_row[:, lanes] * (acc[:, lanes] + part)).astype(bf16)

    for head in range(heads):
        spot = ho.at[partner, head]
        send(spot, spot, sent_p.at[head], recv_p.at[head], on_mesh(tp=partner)).wait_recv()
    multiply([(col, 0, heads), (partner, 0, heads)], first_part)
    def far_arrive(head):
        for r, src in enumerate(far):
            spot = ho.at[src, head]
            send(spot, spot, sent_y.at[head, r], recv_y.at[head, src], on_mesh(tp=src)).wait_recv()
            relay_copy(head, r).start()

    def relay_arrive(head):
        for r, src in enumerate(far_partner):
            spot = ho.at[src, head]
            send(spot, spot, sent_r.at[head, r], recv_r.at[head, src], on_mesh(tp=partner)).wait_recv()

    for members in teams[:-1]:
        for head in members:
            far_arrive(head)
        for head in members:
            relay_arrive(head)
        multiply([(src, members[0], len(members)) for src in far + far_partner], middle_part)
    for head in teams[-1]:
        far_arrive(head)
        if head < heads - 1:
            relay_arrive(head)
            multiply([(src, head, 1) for src in far + far_partner], middle_part)
        else:
            multiply([(src, head, 1) for src in far], middle_part)
            relay_arrive(head)
            multiply([(src, head, 1) for src in far_partner], last_part)
    for copy in out:
        copy.wait_send()
    for item in range(items):
        owner, slot = item // per, item % per

        @pl.when(owner != me)
        def _():
            for copy in ctx_copies(item, me, slot, on_mesh(sp=owner)):
                copy.wait_send()

    for slot in range(per):
        item = me * per + slot

        @pl.when(item < items)
        def _():
            for j in range(2):
                device, copy = zero_copy(slot, item, j)

                @pl.when(device != me)
                def _():
                    copy.wait_send()

    for head in range(heads):
        map_copy(head, out_step).wait_send()

        @pl.when(rank_block(one_way) < blocks_here - 1)
        def _():
            for j in range(2):
                hop_copy(head, j).wait_send()

        for r in range(chips - 1):
            far_copy(head, r).wait_send()
            relay_copy(head, r).wait_send()
        partner_copy(head).wait_send()


def body(
    latent,
    context,
    condition,
    context_condition,
    shift_weight,
    scale_weight,
    gate_weight,
    norm_gain,
    query_weight,
    key_weight,
    value_weight,
    write_weight,
    decay_weight,
    write_bias,
    decay_bias,
    log_rate,
    head_gain,
    out_weight,
):
    sp, tp = lax.axis_size("sp"), lax.axis_size("tp")
    tokens, depth = latent.shape
    ctx_tokens = context.shape[0]
    rows = tokens + ctx_tokens
    out_width = query_weight.shape[1]
    heads = out_width // HEAD_DIM
    items = 2 * heads
    per = -(-items // sp)
    width = out_weight.shape[1]
    chunks = tokens // min(CHUNK, tokens)
    gate_rows = 2 * write_bias.shape[1]
    vmem = pl.BlockSpec(memory_space=pltpu.VMEM)
    anywhere = pl.BlockSpec(memory_space=pl.ANY)
    dma = pltpu.SemaphoreType.DMA
    square, wide = (HEAD_DIM, HEAD_DIM), (HEAD_DIM, 2 * HEAD_DIM)
    scratch = [
        ((3,) + shift_weight.shape, bf16),
        ((rows, depth), bf16),
        ((depth, 3 * out_width), bf16),
        ((2 * gate_rows, depth), bf16),
        (out_weight.shape, bf16),
        ((rows, 128), f32),
        ((rows, depth), bf16),
        ((tokens, out_width), bf16),
        ((rows, out_width), bf16),
        ((rows, out_width), bf16),
        ((sp, 8, width), bf16),
        ((tp, 4, width), f32),
        ((1, width), f32),
        ((heads, rows, 128), f32),
        ((heads, 8, tokens), f32),
        ((heads, 1, tokens), f32),
        ((heads, chunks, 2, tokens // chunks, 2 * HEAD_DIM), bf16),
        ((heads, chunks, 2) + wide, bf16),
        ((heads, 2) + wide, bf16),
        ((heads, tokens, HEAD_DIM), f32),
        ((heads, tokens, 2 * HEAD_DIM), bf16),
        ((items, 8, 128), f32),
        ((per, sp, ctx_tokens, HEAD_DIM), bf16),
        ((per, sp, ctx_tokens, HEAD_DIM), bf16),
        ((per, sp, 8, 128), f32),
        ((per,) + square, bf16),
        ((heads,) + wide, bf16),
        ((heads,) + wide, f32),
        ((heads, 2) + square, bf16),
        ((heads, 2) + square, bf16),
        ((heads,) + square, bf16),
        ((tp, heads, tokens, HEAD_DIM), bf16),
        ((tokens, width), f32),
    ]
    semaphores = [
        (11,), (sp,), (sp,), (tp,), (tp,), (items, 3), (per, sp, 3), (per, 2), (heads, 2), (heads,), (heads,),
        (heads, 2), (heads, tp), (heads, tp), (heads,), (heads,), (heads, tp), (heads, tp),
    ]
    return pl.pallas_call(
        functools.partial(mixer_kernel, sp, tp, heads, per),
        in_specs=[vmem] * 7 + [anywhere] * 11,
        out_specs=vmem,
        out_shape=jax.ShapeDtypeStruct((tokens, width), bf16),
        scratch_shapes=[pltpu.VMEM(shape, dtype) for shape, dtype in scratch] + [dma(shape) for shape in semaphores],
        compiler_params=pltpu.CompilerParams(
            collective_id=0, has_side_effects=True, vmem_limit_bytes=63 * 1024 * 1024
        ),
        name="mixer",
    )(
        condition.reshape(-1, 128),
        context_condition.reshape(-1, 128),
        norm_gain[None, :],
        head_gain[None, :],
        write_bias,
        decay_bias,
        log_rate,
        shift_weight,
        scale_weight,
        gate_weight,
        latent,
        context,
        jnp.transpose(write_weight, (1, 2, 0)).reshape(gate_rows, depth),
        jnp.transpose(decay_weight, (1, 2, 0)).reshape(gate_rows, depth),
        query_weight,
        key_weight,
        value_weight,
        out_weight,
    )


def solution(mesh):
    placed = (
        P("sp", None),
        P("sp", None),
        P("sp"),
        P("sp"),
        P("sp", "tp"),
        P("sp", "tp"),
        P("sp", "tp"),
        P(),
        P(None, "tp"),
        P(None, "tp"),
        P(None, "tp"),
        P(),
        P(),
        P(),
        P(),
        P(),
        P(),
        P(None, "tp"),
    )
    return jax.shard_map(body, mesh=mesh, in_specs=placed, out_specs=P("sp", "tp"), check_vma=False)
```

```python
import functools

import jax
import jax.numpy as jnp
from jax import lax
from jax.experimental import pallas as pl
from jax.experimental.pallas import tpu as pltpu
from jax.sharding import PartitionSpec as P

HEAD_DIM = 128
CHUNK = 128
epsilon = 0.0001
bf16 = jnp.bfloat16
f32 = jnp.float32


def mm(a, b):
    return jnp.dot(a.astype(bf16), b.astype(bf16), preferred_element_type=f32)


def on_mesh(sp=None, tp=None):
    return (lax.axis_index("sp") if sp is None else sp, lax.axis_index("tp") if tp is None else tp)


def send(src, dst, send_sem, recv_sem, device):
    return pltpu.make_async_remote_copy(
        src_ref=src,
        dst_ref=dst,
        send_sem=send_sem,
        recv_sem=recv_sem,
        device_id=device,
        device_id_type=pl.DeviceIdType.MESH,
    )


def greet(devices):
    barrier = pltpu.get_barrier_semaphore()
    for device in devices:
        pl.semaphore_signal(barrier, inc=1, device_id=device, device_id_type=pl.DeviceIdType.MESH)


def grid_iota(size):
    return (
        lax.broadcasted_iota(jnp.int32, (size, size), 0),
        lax.broadcasted_iota(jnp.int32, (size, size), 1),
    )


def bits(mask):
    return mask.astype(f32).astype(bf16)


def half_masks(size):
    half = size // 2
    lanes = lax.broadcasted_iota(jnp.int32, (half, size), 1)
    return bits(lanes < half), bits(lanes >= half)


def spread(compact, masks):
    return jnp.concatenate([compact * masks[0], compact * masks[1]], axis=0)


def invert_halves(items):
    for item in items:
        size = item["system"].shape[0]
        half = size // 2
        item["masks"] = half_masks(size)
        item["system"] = item["system"].astype(bf16)
        item["pieces"] = item["system"][:half] * item["masks"][0] + item["system"][half:] * item["masks"][1]
        rows = lax.broadcasted_iota(jnp.int32, (half, size), 0)
        cols = lax.rem(lax.broadcasted_iota(jnp.int32, (half, size), 1), half)
        item["grid"] = (rows, cols)
        item["inv"] = bits(rows == cols) - item["pieces"] * bits((rows // 2) == (cols // 2))
    step = 2
    while step < max(item["inv"].shape[0] for item in items):
        firsts = []
        active = [item for item in items if step < item["inv"].shape[0]]
        for item in active:
            rows, cols = item["grid"]
            late, early = item["order"](rows, cols)
            late, early = late // step, early // step
            mask = bits(((late % 2) == 1) & (early == late - 1))
            firsts.append(mm(item["pieces"] * mask, spread(item["inv"], item["masks"])).astype(bf16))
        for item, first in zip(active, firsts):
            item["inv"] = item["inv"] - mm(item["inv"], spread(first, item["masks"])).astype(bf16)
        step *= 2


def solve_halves(items):
    def halves(item):
        half = item["inv"].shape[0]
        first, second = item["masks"]
        return half, first, second

    for item in items:
        half, first, second = halves(item)
        both = item["both"].astype(bf16)
        lead = item["pick"](first, second)
        item["lead"] = mm(item["inv"] * lead, both).astype(bf16)
    for item in items:
        half, first, second = halves(item)
        lead = item["lead"]
        mix = item["pick"](item["system"][half:] * first, item["system"][:half] * second)
        item["rest"] = item["pick"](item["both"][half:], item["both"][:half]) - mm(
            mix, jnp.concatenate([lead, lead], axis=0)
        )
    for item in items:
        half, first, second = halves(item)
        rest = item["rest"].astype(bf16)
        trail = mm(
            item["inv"] * item["pick"](second, first), jnp.concatenate([rest, rest], axis=0)
        ).astype(bf16)
        lead = item["lead"]
        item["solved"] = jnp.concatenate([item["pick"](lead, trail), item["pick"](trail, lead)], axis=0)


def chooser(d):
    if isinstance(d, int):
        return lambda a, b: a if d == 0 else b
    return lambda a, b: jnp.where(d == 0, a, b)


def orderer(d):
    if isinstance(d, int):
        return lambda a, b: (a, b) if d == 0 else (b, a)
    return lambda a, b: (jnp.where(d == 0, a, b), jnp.where(d == 0, b, a))


def key_grams(keys):
    size = keys.shape[0]
    rows, cols = grid_iota(size)
    keys_t = keys.astype(f32).T
    gram = jnp.dot(keys, keys_t.astype(bf16), preferred_element_type=f32)
    diag = jnp.where(rows == cols, gram, 0.0)
    s_col = lax.rsqrt(jnp.sum(diag, axis=1, keepdims=True) + epsilon)
    s_row = lax.rsqrt(jnp.sum(diag, axis=0, keepdims=True) + epsilon)
    return gram * s_col * s_row, keys.astype(f32) * s_col, keys_t * s_row, s_row


def eye_matrix():
    rows, cols = grid_iota(HEAD_DIM)
    return (rows == cols).astype(f32)


def make_item(d, gram, keys, keys_t, values, rate_col, run_col, run_row):
    rows, cols = grid_iota(gram.shape[0])
    order = orderer(d)
    late, early = order(rows, cols)
    decay = jnp.where(late > early, jnp.exp(jnp.minimum(run_col - run_row, 0.0)), 0.0)
    both = jnp.concatenate([values * rate_col, keys * (rate_col * jnp.exp(run_col))], axis=1)
    size = gram.shape[0]
    last = chooser(d)(run_row[:, size - 1 :], run_row[:, :1])
    return dict(
        order=order,
        pick=chooser(d),
        system=gram * decay * rate_col,
        both=both,
        gate=jnp.exp(last),
        late_t=(keys_t * jnp.exp(last - run_row)).astype(bf16),
    )


def latent_items(tokens, span, refs):
    size = min(CHUNK, tokens)
    k_ref, v_ref, col_ref, row_ref, srow_ref = refs[:5]
    items = []
    for at in range(0, tokens, size):
        gram, keys, keys_t, s_row = key_grams(k_ref[at : at + size, :])
        srow_ref[:, at : at + size] = s_row
        values = v_ref[at : at + size, :].astype(f32)
        for d in range(2):
            rate_col = col_ref[at : at + size, span * d : span * d + 1]
            run_col = col_ref[at : at + size, span * (2 + d) : span * (2 + d) + 1]
            run_row = row_ref[2 + d : 3 + d, at : at + size]
            item = make_item(d, gram, keys, keys_t, values, rate_col, run_col, run_row)
            item["d"], item["index"] = d, at // size
            items.append(item)
    return items


def context_items(places, d, k_ref, v_ref, g_ref):
    size = k_ref.shape[1]
    items = []
    for step in range(places):
        place = step + d * (places - 1 - 2 * step)
        gram, keys, keys_t, unused = key_grams(k_ref[place])
        gates = g_ref[place]
        gates_t = gates.T
        items.append(
            make_item(
                d, gram, keys, keys_t, v_ref[place].astype(f32),
                gates_t[:size, 0:1], gates_t[:size, 1:2], gates[1:2, :size],
            )
        )
    return items


def solve_items(items):
    invert_halves(items)
    solve_halves(items)
    for item in items:
        item["late"] = mm(item["late_t"], item["solved"])


def latent_maps(groups):
    eye = eye_matrix()
    chains = []
    for items, refs in groups:
        solved_ref, carry_ref, map_ref = refs[5:]
        for item in items:
            solved_ref[item["index"], item["d"]] = item["solved"]
        for d in range(2):
            chain = [i for i in items if i["d"] == d]
            chains.append((chain if d == 0 else chain[::-1], d, carry_ref, map_ref))
    carries = [None] * len(chains)
    for position in range(len(chains[0][0])):
        for which, (chain, d, carry_ref, map_ref) in enumerate(chains):
            item = chain[position]
            late, gate = item["late"], item["gate"]
            fresh = jnp.concatenate([late[:, :HEAD_DIM], (gate - 1.0) * eye - late[:, HEAD_DIM:]], axis=1)
            if position == 0:
                carries[which] = fresh
            else:
                held = carries[which].astype(bf16)
                carry_ref[item["index"], d] = held
                carries[which] = gate * carries[which] + fresh - mm(late[:, HEAD_DIM:], held)
    for carry, (chain, d, carry_ref, map_ref) in zip(carries, chains):
        map_ref[d] = carry.astype(bf16)


def context_state(items):
    state = items[0]["late"][:, :HEAD_DIM]
    for item in items[1:]:
        late = item["late"]
        state = item["gate"] * state + late[:, :HEAD_DIM] - mm(late[:, HEAD_DIM:], state)
    return state.astype(bf16)


def prepare_outputs(tokens, span, q_ref, k_ref, col_ref, row_ref, srow_ref, solved_ref, carry_ref, o_ref, e_ref):
    size = min(CHUNK, tokens)
    rows, cols = grid_iota(size)
    count = tokens // size
    for index in range(count):
        at = index * size
        raw = q_ref[at : at + size, :]
        queries = raw.astype(f32)
        q_scale = lax.rsqrt(jnp.sum(queries * queries, axis=1, keepdims=True) + epsilon) * HEAD_DIM**-0.5
        queries = queries * q_scale
        score = lax.dot_general(
            raw, k_ref[at : at + size, :], (((1,), (1,)), ((), ())), preferred_element_type=f32
        ) * (q_scale * srow_ref[:, at : at + size])
        total = None
        for d in range(2):
            run_col = col_ref[at : at + size, span * (2 + d) : span * (2 + d) + 1]
            run_row = row_ref[2 + d : 3 + d, at : at + size]
            inside = rows >= cols if d == 0 else rows <= cols
            decay = jnp.where(inside, jnp.exp(jnp.minimum(run_col - run_row, 0.0)), 0.0)
            weighed = mm(score * decay, solved_ref[index, d])
            local = weighed[:, :HEAD_DIM]
            early = queries * jnp.exp(run_col) - weighed[:, HEAD_DIM:]
            if index != (0 if d == 0 else count - 1):
                moved = mm(early, carry_ref[index, d])
                local = local + moved[:, :HEAD_DIM]
                early = early + moved[:, HEAD_DIM:]
            e_ref[at : at + size, d * HEAD_DIM : (d + 1) * HEAD_DIM] = early.astype(bf16)
            total = local if total is None else total + local
        o_ref[at : at + size, :] = total


def log1p_unit(u):
    z = u / (2.0 + u)
    z2 = z * z
    series = 1.0 / 11.0 + 0.0 * z2
    for power in (9, 7, 5, 3, 1):
        series = series * z2 + 1.0 / power
    return 2.0 * z * series


def triangle_sums(lower, parts):
    return sum(jnp.dot(lower, part, preferred_element_type=f32) for part in parts)


def split_three(values):
    high = values.astype(bf16)
    rest = values - high.astype(f32)
    middle = rest.astype(bf16)
    return high, middle, (rest - middle.astype(f32)).astype(bf16)


def mixer_kernel(
    sp, tp, heads, per,
    cond_ref, ctx_cond_ref, gain_ref, head_gain_ref, wb_ref, db_ref, lr_ref,
    shift_ref, scale_ref, gate_ref, latent_ref, context_ref, write_ref, decay_ref,
    wq_ref, wk_ref, wv_ref, wo_ref,
    out_ref,
    mod_w, rows_in, weights, gate_w, wo, rstd, mixed, q_s, k_s, v_s,
    got, blocks, gate_row, cols, rows_g, srow, solved, carry, maps, o_s, e_s,
    ctx_send, ctx_k, ctx_v, ctx_g, s_zero, got_map, pair_map, start_in, start_own, hop_out, ho, acc,
    local_sems, sent_a, recv_a, sent_b, recv_b, sent_c, recv_c, sent_s, recv_s, sent_m, recv_m,
    sent_h, sent_y, recv_y, sent_p, recv_p, sent_r, recv_r,
):
    me, col = lax.axis_index("sp"), lax.axis_index("tp")
    width = shift_ref.shape[1]
    tokens, ctx_tokens = latent_ref.shape[0], context_ref.shape[0]
    total_rows = tokens + ctx_tokens
    depth = latent_ref.shape[1]
    out_width = heads * HEAD_DIM
    items = 2 * heads
    loads = []

    def load(src, dst):
        loads.append(pltpu.make_async_copy(src, dst, local_sems.at[len(loads)]))
        loads[-1].start()
        return loads[-1]

    mods = [load(ref, mod_w.at[i]) for i, ref in enumerate([shift_ref, scale_ref, gate_ref])]
    acts = [
        load(context_ref, rows_in.at[pl.ds(tokens, ctx_tokens)]),
        load(latent_ref, rows_in.at[pl.ds(0, tokens)]),
    ]
    gate_rows = write_ref.shape[0]
    projs = [
        load(write_ref, gate_w.at[pl.ds(0, gate_rows)]),
        load(decay_ref, gate_w.at[pl.ds(gate_rows, gate_rows)]),
    ]
    projs += [
        load(ref, weights.at[:, pl.ds(i * out_width, out_width)]) for i, ref in enumerate([wk_ref, wv_ref, wq_ref])
    ]
    out_load = load(wo_ref, wo)
    rings = [on_mesh(sp=lax.rem(me + r, sp)) for r in range(1, sp)]
    cross = [on_mesh(tp=lax.rem(col + r, tp)) for r in range(1, tp)]
    greet(rings + cross)

    def flat(ref):
        values = ref[...].astype(f32)
        return jnp.concatenate([values[i : i + 1] for i in range(values.shape[0])], axis=1)

    silu = jnp.concatenate([flat(cond_ref), flat(ctx_cond_ref), jnp.zeros((6, cond_ref.size), f32)], axis=0)
    silu = (silu / (1.0 + jnp.exp(-silu))).astype(bf16)
    parts = []
    for i in range(3):
        mods[i].wait()
        parts.append(jnp.dot(silu, mod_w[i], preferred_element_type=f32))
    got[me] = jnp.concatenate(
        [parts[0][0:2], parts[1][0:2], parts[2][0:1], jnp.zeros((3, width), f32)], axis=0
    ).astype(bf16)
    pl.semaphore_wait(pltpu.get_barrier_semaphore(), len(rings) + len(cross))
    out = []
    for r, device in enumerate(rings):
        out.append(send(got.at[me], got.at[me], sent_a.at[r], recv_a.at[me], device))
        out[-1].start()
    for act in acts:
        act.wait()
    step = 16

    def stats(i, unused):
        at = pl.ds(pl.multiple_of(i * step, step), step)
        values = rows_in[at, :].astype(f32)
        mean = jnp.sum(values * values, axis=1, keepdims=True) * (1.0 / depth)
        rstd[at, :] = jnp.broadcast_to(lax.rsqrt(mean + epsilon), (step, 128))
        return unused

    lax.fori_loop(0, total_rows // step, stats, 0)
    for r in range(1, sp):
        src = lax.rem(me + r, sp)
        send(got.at[src], got.at[src], sent_a.at[0], recv_a.at[src], on_mesh(sp=src)).wait_recv()
    summed = got[0].astype(f32)
    for place in range(1, sp):
        summed = summed + got[place].astype(f32)
    blocks[col] = summed[0:4]
    gate_row[...] = summed[4:5]
    for r, device in enumerate(cross):
        out.append(send(blocks.at[col], blocks.at[col], sent_b.at[r], recv_b.at[col], device))
        out[-1].start()
    core = lax.rem(col, 2)
    partner = col + 1 - 2 * core
    chips = tp // 2
    far = [lax.rem(col + 2 * r, tp) for r in range(1, chips)]
    far_partner = [place + 1 - 2 * core for place in far]

    def block_arrive(src):
        send(blocks.at[src], blocks.at[src], sent_b.at[0], recv_b.at[src], on_mesh(tp=src)).wait_recv()

    def modulate_rows(place, start, count, index):
        lanes = pl.ds(pl.multiple_of(place * width, width), width)
        block = blocks[place]
        slope = gain_ref[:, lanes] * (1.0 + block[2 + index : 3 + index])
        shift = block[index : index + 1]

        def modulate(i, unused):
            at = pl.ds(pl.multiple_of(start + i * step, step), step)
            scale = jnp.concatenate([rstd[at, :]] * (width // 128), axis=1)
            mixed[at, lanes] = (rows_in[at, lanes].astype(f32) * scale * slope + shift).astype(bf16)
            return unused

        lax.fori_loop(0, count // step, modulate, 0)

    modulate_rows(col, tokens, ctx_tokens, 1)
    modulate_rows(col, 0, tokens, 0)
    block_arrive(partner)
    modulate_rows(partner, tokens, ctx_tokens, 1)
    modulate_rows(partner, 0, tokens, 0)
    for place in far + far_partner:
        block_arrive(place)
        modulate_rows(place, tokens, ctx_tokens, 1)

    tile = 256 if out_width % 256 == 0 else 128

    def project(first, count, which, ref, base):
        def columns(j, unused):
            lanes = pl.ds(pl.multiple_of(which * out_width + j * tile, tile), tile)
            part = jnp.dot(mixed[pl.ds(first, count), :], weights[:, lanes], preferred_element_type=f32)
            ref[pl.ds(first, count), pl.ds(pl.multiple_of(j * tile, tile), tile)] = part.astype(bf16)
            return unused

        lax.fori_loop(0, out_width // tile, columns, 0)

    first_head = col * heads
    span = wb_ref.shape[1]
    bias = jnp.concatenate([wb_ref[0:1], wb_ref[1:2], db_ref[0:1], db_ref[1:2]], axis=1)
    rates = jnp.concatenate([lr_ref[0:1], lr_ref[1:2]] * 2, axis=1)
    lanes_here = bias.shape[1]

    def make_gates(first, count, size):
        pre = lax.dot_general(
            mixed[pl.ds(first, count), :], gate_w[...], (((1,), (1,)), ((), ())), preferred_element_type=f32
        ).astype(bf16).astype(f32) + bias
        rate = 1.0 / (1.0 + jnp.exp(-pre))
        decay = -jnp.exp(rates) * (jnp.maximum(pre, 0.0) + log1p_unit(jnp.exp(-jnp.abs(pre))))
        lane = lax.broadcasted_iota(jnp.int32, (count, lanes_here), 1)
        rows, columns = grid_iota(size)
        lower, upper = (rows >= columns).astype(bf16), (rows <= columns).astype(bf16)
        backward = lax.broadcasted_iota(jnp.int32, (size, lanes_here), 1) >= 3 * span
        running = []
        for at in range(0, count, size):
            split = split_three(decay[at : at + size])
            running.append(jnp.where(backward, triangle_sums(upper, split), triangle_sums(lower, split)))
        gates = jnp.where(lane < 2 * span, rate, jnp.concatenate(running, axis=0))
        gates = jnp.concatenate([gates, jnp.zeros((count, 128 - lanes_here), f32)], axis=1)
        gates = pltpu.roll(gates, lax.rem(128 - first_head, 128), 1)
        for head in range(heads):
            cols[head, pl.ds(first, count), :] = gates if head == 0 else pltpu.roll(gates, 128 - head, 1)
        return gates

    for proj in projs[:2]:
        proj.wait()
    ctx_gates = make_gates(tokens, ctx_tokens, ctx_tokens)
    if ctx_tokens < 128:
        ctx_gates = jnp.concatenate([ctx_gates, jnp.zeros((128 - ctx_tokens, 128), f32)], axis=0)
    gates_t = ctx_gates.T
    for item in range(items):
        head, d = item // 2, item % 2
        ctx_send[item] = jnp.concatenate(
            [
                gates_t[span * d + head : span * d + head + 1],
                gates_t[span * (2 + d) + head : span * (2 + d) + head + 1],
                jnp.zeros((6, 128), f32),
            ],
            axis=0,
        )
    for proj in projs[2:4]:
        proj.wait()
    project(tokens, ctx_tokens, 0, k_s, 0)
    project(tokens, ctx_tokens, 1, v_s, 0)

    def ctx_copies(item, place, slot, device):
        lanes = pl.ds((item // 2) * HEAD_DIM, HEAD_DIM)
        at = pl.ds(tokens, ctx_tokens)
        pairs = [
            (k_s.at[at, lanes], ctx_k.at[slot, place]),
            (v_s.at[at, lanes], ctx_v.at[slot, place]),
            (ctx_send.at[item], ctx_g.at[slot, place]),
        ]
        return [
            send(src, dst, sent_c.at[item, j], recv_c.at[slot, place, j], device) for j, (src, dst) in enumerate(pairs)
        ]

    for item in range(items):
        owner, slot = item // per, item % per

        @pl.when(owner != me)
        def _():
            for copy in ctx_copies(item, me, slot, on_mesh(sp=owner)):
                copy.start()

        @pl.when(owner == me)
        def _():
            lanes = slice((item // 2) * HEAD_DIM, (item // 2 + 1) * HEAD_DIM)
            ctx_k[slot, me] = k_s[tokens : tokens + ctx_tokens, lanes]
            ctx_v[slot, me] = v_s[tokens : tokens + ctx_tokens, lanes]
            ctx_g[slot, me] = ctx_send[item]

    for place in far + far_partner:
        modulate_rows(place, 0, tokens, 0)
    size = min(CHUNK, tokens)
    gates = make_gates(0, tokens, size)
    for j in range(out_width // tile):
        lanes = slice(j * tile, (j + 1) * tile)
        k_s[0:tokens, lanes] = jnp.dot(mixed[0:tokens, :], weights[:, lanes], preferred_element_type=f32).astype(bf16)
    for at in range(0, tokens, 128):
        block_t = gates[at : at + 128].T
        for head in range(heads):
            rows_g[head, :, at : at + 128] = jnp.concatenate(
                [
                    block_t[base + head : base + head + 1] for base in range(0, 4 * span, span)
                ]
                + [jnp.zeros((4, 128), f32)],
                axis=0,
            )
    project(0, tokens, 1, v_s, 0)

    blocks_here = sp // 2
    one_way = lax.rem(me + 1, 2)
    other_way = 1 - one_way

    def lanes_of(head):
        return pl.ds(pl.multiple_of(head * HEAD_DIM, HEAD_DIM), HEAD_DIM)

    def map_copy(head, towards):
        d = other_way
        return send(
            maps.at[head, d], got_map.at[head], sent_m.at[head], recv_m.at[head], on_mesh(sp=me + towards)
        )

    out_step = 1 - 2 * other_way
    in_step = 1 - 2 * one_way

    def refs_of(head):
        lanes = lanes_of(head)
        return (
            k_s.at[:, lanes], v_s.at[:, lanes], cols.at[head], rows_g.at[head], srow.at[head],
            solved.at[head], carry.at[head], maps.at[head],
        )

    def stage_a(members, extra=()):
        groups = [(latent_items(tokens, span, refs_of(head)), refs_of(head)) for head in members]
        solve_items([item for group, unused in groups for item in group] + list(extra))
        latent_maps(groups)
        for head in members:
            map_copy(head, out_step).start()

    def stage_b(members):
        for head in members:
            lanes = lanes_of(head)
            prepare_outputs(
                tokens,
                span,
                q_s.at[:, lanes],
                k_s.at[:, lanes],
                cols.at[head],
                rows_g.at[head],
                srow.at[head],
                solved.at[head],
                carry.at[head],
                o_s.at[head],
                e_s.at[head],
            )

    def stage_pair(members):
        for head in members:
            map_copy(head, -in_step).wait_recv()
        for head in members:
            theirs, mine = got_map[head], maps[head, one_way]
            pair_map[head] = (
                theirs.astype(f32)
                + mine.astype(f32)
                + jnp.dot(mine[:, HEAD_DIM:], theirs, preferred_element_type=f32)
            )

    def first_devices(d):
        return [d * (sp - 1) + (1 - 2 * d) * i for i in range(2)]

    def zero_copy(slot, item, j):
        head, d = item // 2, lax.rem(item, 2)
        return first_devices(d)[j], send(
            s_zero.at[slot],
            start_in.at[head, d],
            sent_s.at[slot, j],
            recv_s.at[head, d],
            on_mesh(sp=first_devices(d)[j]),
        )

    def context_wait(slot):
        for r in range(1, sp):
            src = lax.rem(me + r, sp)
            for j, spot in enumerate((ctx_k.at[slot, src], ctx_v.at[slot, src], ctx_g.at[slot, src])):
                send(spot, spot, sent_c.at[0, j], recv_c.at[slot, src, j], on_mesh(sp=src)).wait_recv()

    def context_parts(slot, item):
        return context_items(sp, lax.rem(item, 2), ctx_k.at[slot], ctx_v.at[slot], ctx_g.at[slot])

    def context_ship(slot, item, state):
        s_zero[slot] = state
        for j in range(2):
            device, copy = zero_copy(slot, item, j)

            @pl.when(device != me)
            def _():
                copy.start()

            @pl.when(device == me)
            def _():
                start_in[item // 2, lax.rem(item, 2)] = state

    def rank_block(d):
        return (d * (sp - 1) + (1 - 2 * d) * me) // 2

    def hop_copy(head, j):
        d = one_way
        return send(
            hop_out.at[head],
            start_in.at[head, d],
            sent_h.at[head, j],
            recv_s.at[head, d],
            on_mesh(sp=me + in_step * (2 - j)),
        )

    def stage_state(members, d):
        block = rank_block(d)
        moving = (d == one_way) & (block < blocks_here - 1)
        for head in members:
            owner = (2 * head + d) // per

            @pl.when((block > 0) | (owner != me))
            def _():
                spot = start_in.at[head, d]
                send(spot, spot, sent_h.at[head, 0], recv_s.at[head, d], on_mesh(sp=lax.rem(me + 1, sp))).wait_recv()

            @pl.when(moving)
            def _():
                state = start_in[head, d]
                pair = pair_map[head]
                hop_out[head] = (
                    state.astype(f32)
                    + pair[:, :HEAD_DIM]
                    + jnp.dot(pair[:, HEAD_DIM:].astype(bf16), state, preferred_element_type=f32)
                ).astype(bf16)
                hop_copy(head, 0).start()

        @pl.when(moving)
        def _():
            for head in members:
                hop_copy(head, 1).start()

        @pl.when(d == one_way)
        def _():
            for head in members:
                state, theirs = start_in[head, d], got_map[head]
                start_own[head, d] = (
                    state.astype(f32)
                    + theirs[:, :HEAD_DIM].astype(f32)
                    + jnp.dot(theirs[:, HEAD_DIM:], state, preferred_element_type=f32)
                ).astype(bf16)

        @pl.when(d != one_way)
        def _():
            for head in members:
                start_own[head, d] = start_in[head, d]

    def far_copy(head, r):
        spot = ho.at[col, head]
        return send(spot, spot, sent_y.at[head, r], recv_y.at[head, col], on_mesh(tp=far[r]))

    def partner_copy(head):
        spot = ho.at[col, head]
        return send(spot, spot, sent_p.at[head], recv_p.at[head], on_mesh(tp=partner))

    def relay_copy(head, r):
        spot = ho.at[far[r], head]
        return send(spot, spot, sent_r.at[head, r], recv_r.at[head, far[r]], on_mesh(tp=partner))

    def stage_final(head):
        states = jnp.concatenate([start_own[head, 0], start_own[head, 1]], axis=0)
        combined = o_s[head] + jnp.dot(e_s[head], states, preferred_element_type=f32)
        scale = lax.rsqrt(jnp.mean(combined * combined, axis=1, keepdims=True) + epsilon)
        ho[col, head] = (combined * scale * head_gain_ref[...]).astype(bf16)
        for r in range(chips - 1):
            far_copy(head, r).start()
        partner_copy(head).start()

    first_dir = jnp.where(me < sp // 2, 0, 1)
    near_block = rank_block(first_dir)
    far_block = blocks_here - 1 - near_block

    def near_event(members):
        for head in members:
            stage_state([head], first_dir)

    def far_event(members):
        for head in members:
            stage_state([head], 1 - first_dir)
            stage_final(head)

    team = 2 if heads % 2 == 0 else 1
    teams = [list(range(at, at + team)) for at in range(0, heads, team)]
    for index, members in enumerate(teams):
        if index == 0 and items == per * sp:
            for slot in range(per):
                context_wait(slot)
            extras = [context_parts(slot, me * per + slot) for slot in range(per)]
            stage_a(members, [item for extra in extras for item in extra])
            for slot, extra in enumerate(extras):
                context_ship(slot, me * per + slot, context_state(extra))
        elif index == 0:
            stage_a(members)
            for slot in range(per):
                item = me * per + slot

                @pl.when(item < items)
                def _():
                    context_wait(slot)
                    extra = context_parts(slot, item)
                    solve_items(extra)
                    context_ship(slot, item, context_state(extra))
        else:
            stage_a(members)
            for head in teams[index - 1]:
                stage_pair([head])

                @pl.when(near_block == 0)
                def _():
                    near_event([head])

    projs[4].wait()
    project(0, tokens, 2, q_s, 0)
    for head in teams[-1]:
        stage_pair([head])

        @pl.when(near_block == 0)
        def _():
            near_event([head])

    @pl.when(near_block > 0)
    def _():
        near_event(teams[0])

    for members in teams:
        stage_b(members)

    @pl.when(near_block > 0)
    def _():
        for members in teams[1:]:
            near_event(members)

    for members in teams:
        far_event(members)
    out_load.wait()
    def multiply(spans, finish):
        def columns(j, unused):
            lanes = pl.ds(pl.multiple_of(j * tile, tile), tile)
            part = None
            for src, first, count in spans:
                block = jnp.concatenate([ho[src, first + i] for i in range(count)], axis=1)
                at = pl.ds(pl.multiple_of(src * out_width + first * HEAD_DIM, HEAD_DIM), count * HEAD_DIM)
                term = jnp.dot(block, wo[at, lanes], preferred_element_type=f32)
                part = term if part is None else part + term
            finish(j, lanes, part)
            return unused

        lax.fori_loop(0, width // tile, columns, 0)

    def first_part(j, lanes, part):
        acc[:, lanes] = part

    def middle_part(j, lanes, part):
        acc[:, lanes] = acc[:, lanes] + part

    def last_part(j, lanes, part):
        residual = rows_in[pl.ds(0, tokens), pl.ds(pl.multiple_of(col * width + j * tile, tile), tile)].astype(f32)
        out_ref[:, lanes] = (residual + gate_row[:, lanes] * (acc[:, lanes] + part)).astype(bf16)

    for head in range(heads):
        spot = ho.at[partner, head]
        send(spot, spot, sent_p.at[head], recv_p.at[head], on_mesh(tp=partner)).wait_recv()
    multiply([(col, 0, heads), (partner, 0, heads)], first_part)
    def far_arrive(head):
        for r, src in enumerate(far):
            spot = ho.at[src, head]
            send(spot, spot, sent_y.at[head, r], recv_y.at[head, src], on_mesh(tp=src)).wait_recv()
            relay_copy(head, r).start()

    def relay_arrive(head):
        for r, src in enumerate(far_partner):
            spot = ho.at[src, head]
            send(spot, spot, sent_r.at[head, r], recv_r.at[head, src], on_mesh(tp=partner)).wait_recv()

    for members in teams[:-1]:
        for head in members:
            far_arrive(head)
        for head in members:
            relay_arrive(head)
        multiply([(src, members[0], len(members)) for src in far + far_partner], middle_part)
    for head in teams[-1]:
        far_arrive(head)
        if head < heads - 1:
            relay_arrive(head)
            multiply([(src, head, 1) for src in far + far_partner], middle_part)
        else:
            multiply([(src, head, 1) for src in far], middle_part)
            relay_arrive(head)
            multiply([(src, head, 1) for src in far_partner], last_part)
    for copy in out:
        copy.wait_send()
    for item in range(items):
        owner, slot = item // per, item % per

        @pl.when(owner != me)
        def _():
            for copy in ctx_copies(item, me, slot, on_mesh(sp=owner)):
                copy.wait_send()

    for slot in range(per):
        item = me * per + slot

        @pl.when(item < items)
        def _():
            for j in range(2):
                device, copy = zero_copy(slot, item, j)

                @pl.when(device != me)
                def _():
                    copy.wait_send()

    for head in range(heads):
        map_copy(head, out_step).wait_send()

        @pl.when(rank_block(one_way) < blocks_here - 1)
        def _():
            for j in range(2):
                hop_copy(head, j).wait_send()

        for r in range(chips - 1):
            far_copy(head, r).wait_send()
            relay_copy(head, r).wait_send()
        partner_copy(head).wait_send()


def body(
    latent,
    context,
    condition,
    context_condition,
    shift_weight,
    scale_weight,
    gate_weight,
    norm_gain,
    query_weight,
    key_weight,
    value_weight,
    write_weight,
    decay_weight,
    write_bias,
    decay_bias,
    log_rate,
    head_gain,
    out_weight,
):
    sp, tp = lax.axis_size("sp"), lax.axis_size("tp")
    tokens, depth = latent.shape
    ctx_tokens = context.shape[0]
    rows = tokens + ctx_tokens
    out_width = query_weight.shape[1]
    heads = out_width // HEAD_DIM
    items = 2 * heads
    per = -(-items // sp)
    width = out_weight.shape[1]
    chunks = tokens // min(CHUNK, tokens)
    gate_rows = 2 * write_bias.shape[1]
    vmem = pl.BlockSpec(memory_space=pltpu.VMEM)
    anywhere = pl.BlockSpec(memory_space=pl.ANY)
    dma = pltpu.SemaphoreType.DMA
    square, wide = (HEAD_DIM, HEAD_DIM), (HEAD_DIM, 2 * HEAD_DIM)
    scratch = [
        ((3,) + shift_weight.shape, bf16),
        ((rows, depth), bf16),
        ((depth, 3 * out_width), bf16),
        ((2 * gate_rows, depth), bf16),
        (out_weight.shape, bf16),
        ((rows, 128), f32),
        ((rows, depth), bf16),
        ((tokens, out_width), bf16),
        ((rows, out_width), bf16),
        ((rows, out_width), bf16),
        ((sp, 8, width), bf16),
        ((tp, 4, width), f32),
        ((1, width), f32),
        ((heads, rows, 128), f32),
        ((heads, 8, tokens), f32),
        ((heads, 1, tokens), f32),
        ((heads, chunks, 2, tokens // chunks, 2 * HEAD_DIM), bf16),
        ((heads, chunks, 2) + wide, bf16),
        ((heads, 2) + wide, bf16),
        ((heads, tokens, HEAD_DIM), f32),
        ((heads, tokens, 2 * HEAD_DIM), bf16),
        ((items, 8, 128), f32),
        ((per, sp, ctx_tokens, HEAD_DIM), bf16),
        ((per, sp, ctx_tokens, HEAD_DIM), bf16),
        ((per, sp, 8, 128), f32),
        ((per,) + square, bf16),
        ((heads,) + wide, bf16),
        ((heads,) + wide, f32),
        ((heads, 2) + square, bf16),
        ((heads, 2) + square, bf16),
        ((heads,) + square, bf16),
        ((tp, heads, tokens, HEAD_DIM), bf16),
        ((tokens, width), f32),
    ]
    semaphores = [
        (11,), (sp,), (sp,), (tp,), (tp,), (items, 3), (per, sp, 3), (per, 2), (heads, 2), (heads,), (heads,),
        (heads, 2), (heads, tp), (heads, tp), (heads,), (heads,), (heads, tp), (heads, tp),
    ]
    return pl.pallas_call(
        functools.partial(mixer_kernel, sp, tp, heads, per),
        in_specs=[vmem] * 7 + [anywhere] * 11,
        out_specs=vmem,
        out_shape=jax.ShapeDtypeStruct((tokens, width), bf16),
        scratch_shapes=[pltpu.VMEM(shape, dtype) for shape, dtype in scratch] + [dma(shape) for shape in semaphores],
        compiler_params=pltpu.CompilerParams(
            collective_id=0, has_side_effects=True, vmem_limit_bytes=63 * 1024 * 1024
        ),
        name="mixer",
    )(
        condition.reshape(-1, 128),
        context_condition.reshape(-1, 128),
        norm_gain[None, :],
        head_gain[None, :],
        write_bias,
        decay_bias,
        log_rate,
        shift_weight,
        scale_weight,
        gate_weight,
        latent,
        context,
        jnp.transpose(write_weight, (1, 2, 0)).reshape(gate_rows, depth),
        jnp.transpose(decay_weight, (1, 2, 0)).reshape(gate_rows, depth),
        query_weight,
        key_weight,
        value_weight,
        out_weight,
    )


def solution(mesh):
    placed = (
        P("sp", None),
        P("sp", None),
        P("sp"),
        P("sp"),
        P("sp", "tp"),
        P("sp", "tp"),
        P("sp", "tp"),
        P(),
        P(None, "tp"),
        P(None, "tp"),
        P(None, "tp"),
        P(),
        P(),
        P(),
        P(),
        P(),
        P(),
        P(None, "tp"),
    )
    return jax.shard_map(body, mesh=mesh, in_specs=placed, out_specs=P("sp", "tp"), check_vma=False)
```
